512 devices in a mesh: fs: 128 (over z, x, core), tp: 4 (over y).
Axes of the slice: x: 4, y: 4, z: 16, core: 2. Of those that a mesh axis runs over, the one named last changes fastest.
Arguments:
- block_input: bfloat16 [131072, 2048], P(('fs', 'tp')), may hold values from -6 to 6
- gate_cotangent: bfloat16 [131072, 2048], P('fs', 'tp'), may hold values from -0.016479492 to 0.016479492
- gated_state: bfloat16 [131072, 2048], P('fs', 'tp'), may hold values from -6 to 6
- mixer_cotangent: bfloat16 [131072, 2048], P(('fs', 'tp')), may hold values from -0.016479492 to 0.016479492
- gate_basis: bfloat16 [2048, 512], P('fs'), may hold values from -0.125 to 0.125
- out_basis: bfloat16 [2048, 512], P('fs'), may hold values from -0.125 to 0.125
- gate_master: float32 [2048, 2048], P('fs', 'tp'), may hold values from -0.6 to 0.6
- out_master: float32 [2048, 2048], P('tp', 'fs'), may hold values from -0.6 to 0.6
- gate_first: float32 [512, 2048], P('fs', 'tp'), may hold values from -3 to 3
- gate_second: float32 [512, 2048], P('fs', 'tp'), may hold values from 0.01 to 8.1, as said below
- out_first: float32 [512, 2048], P('fs', 'tp'), may hold values from -3 to 3
- out_second: float32 [512, 2048], P('fs', 'tp'), may hold values from 0.01 to 8.1, as said below
Outputs:
- gate_master_new: float32 [2048, 2048], P('fs', 'tp')
- out_master_new: float32 [2048, 2048], P('tp', 'fs')
- gate_copy: bfloat16 [2048, 2048], P(None, 'tp')
- out_copy: bfloat16 [2048, 2048], P('tp')
- gate_first_new: float32 [512, 2048], P('fs', 'tp')
- gate_second_new: float32 [512, 2048], P('fs', 'tp')
- out_first_new: float32 [512, 2048], P('fs', 'tp')
- out_second_new: float32 [512, 2048], P('fs', 'tp')
The draws below stay inside these ranges and needn't reach their ends.
Inputs may be any that keep to these rules, and one draw needn't show every extreme that they name: `gate_second`: positive. `out_second`: positive.
All inputs are finite; a program needn't handle non-finite values.
Results may differ from the reference program's by a relative error of at most 0.0038.
Values may be sent and summed in bfloat16 or wider, within the bound.
A program may use at most 64 MiB of HBM per device.

```python
import math
import jax
import jax.numpy as jnp
from jax import lax

D = 2048
DI = 2048
R = 512
TOKENS = 131072


def second_moment(key):
    row_frac = jnp.arange(R, dtype=jnp.float32)[:, None] / R
    col_frac = jnp.arange(DI, dtype=jnp.float32)[None, :] / DI
    jitter = jax.random.uniform(key, (R, DI), jnp.float32, 0.0, 1.0)
    slope = row_frac + col_frac
    return 0.01 * jnp.exp(jitter * math.log(10.0) + slope * math.log(9.0))


def draw_gate_second(key, part):
    return second_moment(jax.random.fold_in(key, 11))


def draw_out_second(key, part):
    return second_moment(jax.random.fold_in(key, 12))


def levels(stream_key, extent, shards, low, top_value):
    loudness, own = 1.0, jax.random.fold_in(stream_key, 6)
    for axis_at, parts in shards:
        draws = jnp.exp(jax.random.uniform(jax.random.fold_in(own, axis_at), (parts,), jnp.float32, low / len(shards), top_value / len(shards)))
        loudness = loudness * jnp.repeat(draws, extent[axis_at] // parts).reshape([-1 if axis == axis_at else 1 for axis in range(len(extent))])
    return loudness


def gaussian(stream_key, shape, width, bound, split=(), kind=jnp.bfloat16):
    loudness = levels(stream_key, shape, split, -0.22, 0.18) if split else 1.0
    entries = jax.random.normal(stream_key, shape, jnp.float32) * width * loudness
    return jnp.minimum(jnp.maximum(entries, -bound), bound).astype(kind)


def setup_inputs(seed: int = 0) -> dict:
    splits = jax.random.split(jax.random.key(seed), 13)
    return {
        "block_input": gaussian(splits[0], (TOKENS, D), 1.0, 6.0, ((0, 512),)),
        "gate_cotangent": gaussian(splits[1], (TOKENS, DI), (TOKENS ** -0.5), 0.016479492, ((0, 128), (1, 4))),
        "gated_state": gaussian(splits[2], (TOKENS, DI), 1.0, 6.0, ((0, 128), (1, 4))),
        "mixer_cotangent": gaussian(splits[3], (TOKENS, D), (TOKENS ** -0.5), 0.016479492, ((0, 512),)),
        "gate_basis": gaussian(splits[4], (D, R), D ** -0.5, 0.125, ((0, 128),)),
        "out_basis": gaussian(splits[5], (D, R), D ** -0.5, 0.125, ((0, 128),)),
        "gate_master": gaussian(splits[6], (D, DI), 0.1, 0.6, ((0, 128), (1, 4)), jnp.float32),
        "out_master": gaussian(splits[7], (DI, D), 0.1, 0.6, ((0, 4), (1, 128)), jnp.float32),
        "gate_first": gaussian(splits[8], (R, DI), 0.5, 3.0, ((0, 128), (1, 4)), jnp.float32),
        "gate_second": draw_gate_second(jax.random.fold_in(splits[12], 71), 0),
        "out_first": gaussian(splits[10], (R, DI), 0.5, 3.0, ((0, 128), (1, 4)), jnp.float32),
        "out_second": draw_out_second(jax.random.fold_in(splits[12], 71), 0),
    }


def reference(block_input, gate_cotangent, gated_state, mixer_cotangent, gate_basis, out_basis, gate_master, out_master, gate_first, gate_second, out_first, out_second):
    proj_in = jnp.dot(block_input, gate_basis, preferred_element_type=jnp.float32).astype(jnp.bfloat16)
    proj_cot = jnp.dot(mixer_cotangent, out_basis, preferred_element_type=jnp.float32).astype(jnp.bfloat16)
    contract = (((0,), (0,)), ((), ()))
    gate_low = lax.dot_general(proj_in, gate_cotangent, contract, preferred_element_type=jnp.float32)
    out_low = lax.dot_general(proj_cot, gated_state, contract, preferred_element_type=jnp.float32)
    gate_first_new = 0.9 * gate_first + 0.1 * gate_low
    out_first_new = 0.9 * out_first + 0.1 * out_low
    gate_second_new = 0.95 * gate_second + 0.05 * gate_low * gate_low
    out_second_new = 0.95 * out_second + 0.05 * out_low * out_low
    gate_raw = gate_first_new / jnp.sqrt(gate_second_new)
    out_raw = out_first_new / jnp.sqrt(out_second_new)
    squares = jnp.sum(gate_raw * gate_raw) + jnp.sum(out_raw * out_raw)
    norm_scale = lax.rsqrt(squares / (2.0 * R * DI) + 1e-06)
    gate_update = jnp.dot(gate_basis.astype(jnp.float32), gate_raw * norm_scale, precision=lax.Precision.HIGHEST)
    out_update = lax.dot_general(out_raw * norm_scale, out_basis.astype(jnp.float32), (((0,), (1,)), ((), ())), precision=lax.Precision.HIGHEST)
    gate_master_new = gate_master - 0.25 * gate_update
    out_master_new = out_master - 0.25 * out_update
    return (gate_master_new, out_master_new, gate_master_new.astype(jnp.bfloat16), out_master_new.astype(jnp.bfloat16), gate_first_new, gate_second_new, out_first_new, out_second_new)
```

```python
import functools

import jax
import jax.numpy as jnp
from jax import lax
from jax.experimental import pallas as pl
from jax.experimental.pallas import tpu as pltpu
from jax.sharding import Mesh
from jax.sharding import PartitionSpec as P

MESH = pl.DeviceIdType.MESH
BF = jnp.bfloat16
F32 = jnp.float32
ZN, XN, YN = 16, 4, 4
FSN = ("z", "x", "core")
FS_TP = ("z", "x", "core", "tp")
NC = 4
ZQ = ZN // NC
OWN = 8
NID = ZN


def block_id(sign, dist):
    return 2 * dist - 1 if sign > 0 else 2 * dist


def remote(src, dst, send, recv, **to):
    return pltpu.make_async_remote_copy(
        src_ref=src, dst_ref=dst, send_sem=send, recv_sem=recv, device_id=to, device_id_type=MESH
    )


def kernel(
    low_rank, inner,
    bi, gc, gs, mc, gb, ob, gmb, omb, gm, om, gf, gsec, of, osec,
    gm_out, om_out, gcopy, ocopy, gf_out, gs_out, of_out, os_out,
    X, C, BB, MB, PT, LB, XR, ZS, ZR, RAW, FS, NM, PM, SQ, GO, OO, GM, OM, GMO, OMO,
    li, ss, sr, ms,
    b_zs, b_zr, b_xs, b_xr, b_os, b_or,
    m_zs, m_zr, m_xs, m_xr, m_os, m_or,
    d_s, d_r,
    y_s, y_r, yo_s, yo_r,
    rx_s, rx_r, rz_s, rz_r,
    az_s, az_r, ax_s, ax_r, ad_s, ad_r,
    pm_s, pm_r, sq_s, sq_r, out_s,
):
    z, x, c, y = (lax.axis_index(a) for a in ("z", "x", "core", "tp"))
    other = 1 - c

    def zat(k):
        return lax.rem(z + k + ZN, ZN)

    def xat(k):
        return lax.rem(x + k + XN, XN)

    def yat(k):
        return lax.rem(y + k + YN, YN)

    own_rows = pl.ds(pl.multiple_of(c * 16, 16), 16)
    dsts = (
        lambda m: BB.at[m, z, x, own_rows],
        lambda m: X.at[c],
        lambda m: C.at[c],
        lambda m: MB.at[m, z, x, own_rows],
        lambda m: FS.at[0, c],
        lambda m: FS.at[1, c],
    )
    gates = (gb, bi, gc, gmb, gf, gsec)
    outs = (ob, mc, gs, omb, of, osec)

    def load(mine):
        for k in range(6):
            pltpu.make_async_copy(mine[k], dsts[k](c), li.at[k]).start()

    def ship(theirs):
        for k in range(6):
            remote(theirs[k], dsts[k](other), ss.at[k], sr.at[k], core=other).start()

    pl.when(c == 0)(lambda: load(gates))
    pl.when(c == 1)(lambda: load(outs))
    pltpu.make_async_copy(gm, GM, ms.at[0]).start()
    pltpu.make_async_copy(om, OM, ms.at[1]).start()

    barrier = pltpu.get_barrier_semaphore()
    for k in (1, -1, 2, -2):
        pl.semaphore_signal(barrier, inc=1, device_id={"z": zat(k)}, device_id_type=MESH)
    for k in (1, -1):
        pl.semaphore_signal(barrier, inc=1, device_id={"x": xat(k)}, device_id_type=MESH)
        pl.semaphore_signal(barrier, inc=1, device_id={"tp": yat(k)}, device_id_type=MESH)
    pl.semaphore_signal(barrier, inc=1, device_id={"core": other}, device_id_type=MESH)
    pl.semaphore_wait(barrier, 9)

    pl.when(c == 0)(lambda: ship(outs))
    pl.when(c == 1)(lambda: ship(gates))

    def arrived(k):
        ref = dsts[k](c)
        pltpu.make_async_copy(gates[k], ref, li.at[k]).wait()
        remote(ref, ref, ss.at[k], sr.at[k], core=other).wait_recv()

    def gather(buf, zs, zr, xs, xr, os, orr):
        def zof(i):
            d = (i + 1) // 2
            odd = lax.rem(i, 2)
            return lax.rem(z + ZN + (1 - 2 * odd) * d, ZN)

        def zsends(s):
            for sign, far in ((1, ZN // 2), (-1, ZN // 2 - 1)):
                src = buf.at[zat(-sign * 2 * s), x]
                for k in (2, 1):
                    if 2 * s + k <= far:
                        i = block_id(sign, 2 * s + k)
                        remote(src, src, zs.at[i], zr.at[i], z=zat(sign * k)).start()

        def zwait(i):
            ref = buf.at[zof(i), x]
            remote(ref, ref, zs.at[i], zr.at[i], z=zat(1)).wait_recv()

        def forward(i):
            ref = buf.at[zof(i), x]
            remote(ref, ref, xs.at[0, i], xr.at[0, i], x=xat(1)).start()
            remote(ref, ref, xs.at[1, i], xr.at[1, i], x=xat(-1)).start()

        def halves(i):
            zz = zof(i)
            return buf.at[zz, xat(-1), pl.ds(0, 16)], buf.at[zz, xat(1), pl.ds(16, 16)]

        def relay(i):
            zz = zof(i)
            left, right = buf.at[zz, xat(-1)], buf.at[zz, xat(1)]
            remote(left, left, xs.at[0, i], xr.at[0, i], x=xat(1)).wait_recv()
            remote(right, right, xs.at[1, i], xr.at[1, i], x=xat(-1)).wait_recv()
            a, b = halves(i)
            remote(a, a, os.at[0, i], orr.at[0, i], x=xat(1)).start()
            remote(b, b, os.at[1, i], orr.at[1, i], x=xat(-1)).start()

        def opposite(i):
            zz = zof(i)
            for h in range(2):
                ref = buf.at[zz, xat(2), pl.ds(16 * h, 16)]
                remote(ref, ref, os.at[h, i], orr.at[h, i], x=xat(1)).wait_recv()

        def drain(i):
            zz = zof(i)
            ref = buf.at[zz, x]
            for h in range(2):
                remote(ref, ref, xs.at[h, i], xr.at[h, i], x=xat(1)).wait_send()
                half = buf.at[zz, x, pl.ds(0, 16)]
                remote(half, half, os.at[h, i], orr.at[h, i], x=xat(1)).wait_send()

        def zdrain(i):
            ref = buf.at[z, x]
            remote(ref, ref, zs.at[i], zr.at[i], z=zat(1)).wait_send()

        def each(f, lo, hi):
            def body(i, _):
                f(i)
                return 0
            lax.fori_loop(lo, hi, body, 0)

        def both(lo, hi):
            for i in range(lo, hi):
                zwait(i)
                forward(i)

        def step0():
            zsends(0)
            forward(0)

        def step(s):
            for i in (4 * s - 1, 4 * s):
                zwait(i)
            zsends(s)
            for i in (4 * s - 3, 4 * s - 2):
                zwait(i)
            each(forward, 4 * s - 3, 4 * s + 1)
            each(relay, max(0, 4 * s - 7), 4 * s - 3)

        def step4():
            both(13, 16)
            each(relay, 9, 13)

        def step5():
            each(relay, 13, 16)

        def step6():
            each(opposite, 0, 16)

        def finish():
            each(zdrain, 1, 16)
            each(drain, 0, 16)

        steps = [step0] + [functools.partial(step, s) for s in (1, 2, 3)] + [step4, step5, step6]
        return steps, finish

    basis_steps, basis_finish = gather(BB.at[c], b_zs, b_zr, b_xs, b_xr, b_os, b_or)
    master_steps, master_finish = gather(MB.at[c], m_zs, m_zr, m_xs, m_xr, m_os, m_or)

    arrived(0)
    for step in basis_steps[:4]:
        step()
    arrived(3)
    master_steps[0]()
    for step in basis_steps[4:]:
        step()

    whole = [
        remote(BB.at[c], BB.at[c], d_s.at[0], d_r.at[0], core=other),
        remote(MB.at[c], MB.at[c], d_s.at[1], d_r.at[1], core=other),
    ]
    whole[0].start()

    arrived(1)
    W = low_rank // NC
    tokens = 512

    def y_copies(u):
        ref = PT.at[y, u]
        return [
            remote(ref, ref, y_s.at[0, u], y_r.at[0, u], tp=yat(1)),
            remote(ref, ref, y_s.at[1, u], y_r.at[1, u], tp=yat(-1)),
        ]

    for u in range(NC):
        basis = BB[c, :, :, :, u * W : (u + 1) * W].reshape(ZN * XN * 32, W)
        proj = jnp.dot(X[...].reshape(tokens, -1), basis, preferred_element_type=F32)
        PT[y, u] = proj.T.astype(BF)
        for copy in y_copies(u):
            copy.start()

    master_steps[1]()
    arrived(2)
    arrived(4)
    arrived(5)

    def y_relays(u):
        left, right = PT.at[yat(-1), u], PT.at[yat(1), u]
        a, b = PT.at[yat(-1), u, pl.ds(0, W // 2)], PT.at[yat(1), u, pl.ds(W // 2, W // 2)]
        return (
            remote(left, left, y_s.at[0, u], y_r.at[0, u], tp=yat(1)),
            remote(right, right, y_s.at[1, u], y_r.at[1, u], tp=yat(-1)),
            remote(a, a, yo_s.at[0, u], yo_r.at[0, u], tp=yat(1)),
            remote(b, b, yo_s.at[1, u], yo_r.at[1, u], tp=yat(-1)),
        )

    def y_stage(u):
        l, r, a, b = y_relays(u)
        l.wait_recv()
        a.start()
        r.wait_recv()
        b.start()

    def rx_copies(u):
        return [
            remote(LB.at[u, xat(d)], XR.at[u, d - 1], rx_s.at[u, d - 1], rx_r.at[u, d - 1], x=xat(d))
            for d in (1, 2, 3)
        ]

    def low_stage(u):
        for h in range(2):
            ref = PT.at[yat(2), u, pl.ds(h * (W // 2), W // 2)]
            remote(ref, ref, yo_s.at[h, u], yo_r.at[h, u], tp=yat(1)).wait_recv()

        def add(k, total):
            rows = pl.ds(pl.multiple_of(k * 256, 256), 256)
            for h in range(2):
                total += jnp.dot(
                    PT[k, u, :, h * 256 : (h + 1) * 256], C[h, rows], preferred_element_type=F32
                )
            return total

        total = lax.fori_loop(0, YN, add, jnp.zeros((W, inner), F32))
        LB[u] = total.reshape(XN, ZQ, OWN, inner).astype(BF)
        for copy in rx_copies(u):
            copy.start()

    def rz_copy(u, q):
        to = q * NC + u
        return remote(ZS.at[u, q], ZR.at[z], rz_s.at[u, q], rz_r.at[z], z=to)

    def rx_stage(u):
        total = LB[u, x].astype(F32)
        for d, copy in enumerate(rx_copies(u)):
            copy.wait_recv()
            total += XR[u, d].astype(F32)
        ZS[u] = total.astype(BF)
        for q in range(ZQ):
            pl.when(z != q * NC + u)(lambda: rz_copy(u, q).start())

    zq = z // NC

    def az_copy(u, d):
        ref = RAW.at[c, u, x, zq]
        return remote(ref, ref, az_s.at[d], az_r.at[u, zq], z=zat(d))

    def pm_copy():
        return remote(NM.at[other], PM, pm_s, pm_r, core=other)

    def rz_stage(u):
        @pl.when(lax.rem(z, NC) == u)
        def _():
            def add(d, total):
                src = zat(d)
                ref = ZR.at[src]
                remote(ref, ref, rz_s.at[u, 0], rz_r.at[src], z=src).wait_recv()
                return total + ZR[src].astype(F32)

            low = lax.fori_loop(1, ZN, add, ZS[u, zq].astype(F32))
            raws = []
            for h in range(2):
                part = low[4 * h : 4 * h + 4]
                first = 0.9 * FS[0, h] + 0.1 * part
                second = 0.95 * FS[1, h] + 0.05 * part * part
                NM[h, 0] = first
                NM[h, 1] = second
                raws.append(first / jnp.sqrt(second))
            RAW[c, u, x, zq] = jnp.concatenate(raws, axis=0).astype(BF)

            def send(d, _):
                az_copy(u, d).start()
                return 0

            lax.fori_loop(1, ZN, send, 0)
            pm_copy().start()

    def ax_copies(u):
        ref = RAW.at[c, u, x]
        return [
            remote(ref, ref, ax_s.at[u, d - 1], ax_r.at[u, d - 1], x=xat(d)) for d in (1, 2, 3)
        ]

    def az_stage(u):
        for q in range(ZQ):
            ref = RAW.at[c, u, x, q]
            pl.when(z != q * NC + u)(
                lambda: remote(ref, ref, az_s.at[1], az_r.at[u, q], z=zat(1)).wait_recv()
            )
        for copy in ax_copies(u):
            copy.start()

    def ad_copy(u):
        ref = RAW.at[c, u]
        return remote(ref, ref, ad_s.at[u], ad_r.at[u], core=other)

    def ax_stage(u):
        for d in (1, 2, 3):
            ref = RAW.at[c, u, xat(-d)]
            remote(ref, ref, ax_s.at[u, d - 1], ax_r.at[u, d - 1], x=xat(d)).wait_recv()
        ad_copy(u).start()

    def ad_stage(u):
        ref = RAW.at[other, u]
        remote(ref, ref, ad_s.at[u], ad_r.at[u], core=other).wait_recv()

    stages = ((y_stage, 0), (low_stage, 0), (rx_stage, 1), (rz_stage, 2), (az_stage, 3), (ax_stage, 4))
    late = {0: 2, 1: 3, 2: 4, 3: 5, 4: 6}
    for t in range(NC + 5):
        for stage, lag in stages:
            if 0 <= t - lag < NC:
                stage(t - lag)
        if t in late:
            master_steps[late[t]]()
            if late[t] == 6:
                whole[1].start()
    for u in range(NC):
        ad_stage(u)

    squares = jnp.zeros((8, 128), F32)
    for m in range(2):
        for u in range(NC):
            r = RAW[m, u].reshape(W, inner).astype(F32)
            r = (r * r).reshape(W // 8, 8, inner).sum(axis=0)
            for k in range(inner // 128):
                squares += r[:, k * 128 : (k + 1) * 128]
    SQ[y] = squares

    def sq_copy(d):
        return remote(SQ.at[y], SQ.at[y], sq_s.at[d - 1], sq_r.at[d - 1], tp=yat(d))

    for d in (1, 2, 3):
        sq_copy(d).start()
    for d in (1, 2, 3):
        ref = SQ.at[yat(-d)]
        remote(ref, ref, sq_s.at[d - 1], sq_r.at[d - 1], tp=yat(d)).wait_recv()
    total = jnp.sum(SQ[0] + SQ[1] + SQ[2] + SQ[3])
    scale = 0.25 * lax.rsqrt(
        jnp.full((1, inner), total, F32) / (2.0 * low_rank * inner * YN) + 1e-06
    )

    for k in range(2):
        src = BB.at[other] if k == 0 else MB.at[other]
        remote(src, src, d_s.at[k], d_r.at[k], core=other).wait_recv()

    TILE = 256

    def gate_out(t):
        rows = pl.ds(pl.multiple_of(t * TILE, TILE), TILE)
        return pltpu.make_async_copy(GO.at[rows], gcopy.at[rows], out_s.at[0, t])

    def out_out(t):
        rows = pl.ds(pl.multiple_of(t * 64, 64), 64)
        return pltpu.make_async_copy(OO.at[rows], ocopy.at[rows], out_s.at[1, t])

    raws = [RAW[m].reshape(low_rank, inner) for m in range(2)]

    def tile(t, _):
        zz = pl.ds(t * 2, 2)
        rows = pl.ds(pl.multiple_of(t * TILE, TILE), TILE)
        up = jnp.dot(BB[0, zz].reshape(TILE, low_rank), raws[0], preferred_element_type=F32)
        GO[rows] = (MB[0, zz].reshape(TILE, inner).astype(F32) - scale * up).astype(BF)
        gate_out(t).start()
        up = jnp.dot(BB[1, zz].reshape(TILE, low_rank), raws[1], preferred_element_type=F32)
        new = MB[1, zz].reshape(TILE, inner).astype(F32) - scale * up
        OO[:, rows] = new.T.astype(BF)
        return 0

    lax.fori_loop(0, 8, tile, 0)
    for t in range(8):
        out_out(t).start()

    pltpu.make_async_copy(gm, GM, ms.at[0]).wait()
    pltpu.make_async_copy(om, OM, ms.at[1]).wait()
    up = jnp.dot(BB[0, z, x, own_rows], raws[0], preferred_element_type=F32)
    GMO[...] = GM[...] - scale * up
    up = jnp.dot(BB[1, z, x, own_rows], raws[1], preferred_element_type=F32)
    OMO[...] = OM[...] - scale * up

    remote(PM, PM, pm_s, pm_r, core=other).wait_recv()

    def moments(mine, theirs):
        return [
            pltpu.make_async_copy(GMO, gm_out, ms.at[2]),
            pltpu.make_async_copy(OMO, om_out, ms.at[3]),
            pltpu.make_async_copy(NM.at[c, 0], mine[0], ms.at[4]),
            pltpu.make_async_copy(NM.at[c, 1], mine[1], ms.at[5]),
            pltpu.make_async_copy(PM.at[0], theirs[0], ms.at[6]),
            pltpu.make_async_copy(PM.at[1], theirs[1], ms.at[7]),
        ]

    def write(mine, theirs):
        for copy in moments(mine, theirs):
            copy.start()

    pl.when(c == 0)(lambda: write((gf_out, gs_out), (of_out, os_out)))
    pl.when(c == 1)(lambda: write((of_out, os_out), (gf_out, gs_out)))

    for k in range(6):
        ref = dsts[k](other)
        remote(gates[k], ref, ss.at[k], sr.at[k], core=other).wait_send()
    basis_finish()
    master_finish()
    for copy in whole:
        copy.wait_send()
    for u in range(NC):
        for copy in y_copies(u):
            copy.wait_send()
        _, _, a, b = y_relays(u)
        a.wait_send()
        b.wait_send()
        for copy in rx_copies(u) + ax_copies(u):
            copy.wait_send()
        for q in range(ZQ):
            pl.when(z != q * NC + u)(lambda: rz_copy(u, q).wait_send())
        ad_copy(u).wait_send()

    def sent(d, _):
        az_copy(0, d).wait_send()
        return 0

    lax.fori_loop(1, ZN, sent, 0)
    pm_copy().wait_send()
    for d in (1, 2, 3):
        sq_copy(d).wait_send()
    for t in range(8):
        gate_out(t).wait()
        out_out(t).wait()
    for copy in moments((gf_out, gs_out), (of_out, os_out)):
        copy.wait()


def on_device(
    block_input, gate_cotangent, gated_state, mixer_cotangent, gate_basis, out_basis,
    gate_master, out_master, gate_first, gate_second, out_first, out_second,
):
    low_rank = gate_basis.shape[1]
    inner = gate_first.shape[1]
    rows = gate_basis.shape[0]

    def by_owner(b):
        b = b.reshape(rows, ZQ, NC, XN, OWN)
        return b.transpose(0, 2, 3, 1, 4).reshape(rows, low_rank)

    out_t = out_master.T
    D = pltpu.SemaphoreType.DMA
    V = pltpu.VMEM
    full = rows * ZN * XN * 2
    W = low_rank // NC
    gather_sems = [
        D((NID,)), D((NID,)), D((2, NID)), D((2, NID)), D((2, NID)), D((2, NID)),
    ]
    outs = (
        jax.ShapeDtypeStruct((rows, inner), F32),
        jax.ShapeDtypeStruct((rows, inner), F32),
        jax.ShapeDtypeStruct((full, inner), BF),
        jax.ShapeDtypeStruct((inner, full), BF),
    ) + (jax.ShapeDtypeStruct(gate_first.shape, F32),) * 4
    res = pl.pallas_call(
        functools.partial(kernel, low_rank, inner),
        out_shape=outs,
        in_specs=[pl.BlockSpec(memory_space=pl.ANY)] * 14,
        out_specs=[pl.BlockSpec(memory_space=pl.ANY)] * 8,
        scratch_shapes=[
            V((2, 256, full), BF),
            V((2, 1024, inner), BF),
            V((2, ZN, XN, 32, low_rank), BF),
            V((2, ZN, XN, 32, inner), BF),
            V((YN, NC, W, 512), BF),
            V((NC, XN, ZQ, OWN, inner), BF),
            V((NC, 3, ZQ, OWN, inner), BF),
            V((NC, ZQ, OWN, inner), BF),
            V((ZN, OWN, inner), BF),
            V((2, NC, XN, ZQ, OWN, inner), BF),
            V((2, 2, 4, inner), F32),
            V((2, 2, 4, inner), F32),
            V((2, 4, inner), F32),
            V((YN, 8, 128), F32),
            V((full, inner), BF),
            V((inner, full), BF),
            V((rows, inner), F32),
            V((rows, inner), F32),
            V((rows, inner), F32),
            V((rows, inner), F32),
            D((6,)), D((6,)), D((6,)), D((8,)),
            *gather_sems,
            *gather_sems,
            D((2,)), D((2,)),
            D((2, NC)), D((2, NC)), D((2, NC)), D((2, NC)),
            D((NC, 3)), D((NC, 3)), D((NC, ZQ)), D((ZN,)),
            D((ZN,)), D((NC, ZQ)), D((NC, 3)), D((NC, 3)), D((NC,)), D((NC,)),
            D, D, D((3,)), D((3,)), D((2, 8)),
        ],
        compiler_params=pltpu.CompilerParams(
            collective_id=0, has_side_effects=True, vmem_limit_bytes=60 * 1024 * 1024
        ),
        name="moment_update",
    )(
        block_input, gate_cotangent, gated_state, mixer_cotangent,
        by_owner(gate_basis), by_owner(out_basis),
        gate_master.astype(BF), out_t.astype(BF), gate_master, out_t,
        gate_first, gate_second, out_first, out_second,
    )
    return (res[0], res[1].T, *res[2:])


def solution(mesh):
    finer = Mesh(mesh.devices.reshape(ZN, XN, 2, mesh.shape["tp"]), FS_TP)
    in_specs = (
        P(FS_TP, None), P(FSN, "tp"), P(FSN, "tp"), P(FS_TP, None), P(FSN, None), P(FSN, None),
        P(FSN, "tp"), P("tp", FSN), P(FSN, "tp"), P(FSN, "tp"), P(FSN, "tp"), P(FSN, "tp"),
    )
    out_specs = (
        P(FSN, "tp"), P("tp", FSN), P(None, "tp"), P("tp", None),
        P(FSN, "tp"), P(FSN, "tp"), P(FSN, "tp"), P(FSN, "tp"),
    )
    return jax.shard_map(
        on_device, mesh=finer, in_specs=in_specs, out_specs=out_specs, check_vma=False
    )
```

```python
import functools

import jax
import jax.numpy as jnp
from jax import lax
from jax.experimental import pallas as pl
from jax.experimental.pallas import tpu as pltpu
from jax.sharding import Mesh
from jax.sharding import PartitionSpec as P

MESH = pl.DeviceIdType.MESH
BF = jnp.bfloat16
F32 = jnp.float32
ZN, XN, YN = 16, 4, 4
FSN = ("z", "x", "core")
FS_TP = ("z", "x", "core", "tp")
NC = 4
ZQ = ZN // NC
OWN = 8
LIMIT1 = 32 * 1024 * 1024
LIMIT2 = 24 * 1024 * 1024
NID = ZN


def block_id(sign, dist):
    return 2 * dist - 1 if sign > 0 else 2 * dist


def remote(src, dst, send, recv, **to):
    return pltpu.make_async_remote_copy(
        src_ref=src, dst_ref=dst, send_sem=send, recv_sem=recv, device_id=to, device_id_type=MESH
    )


def kernel(
    low_rank, inner,
    bi, gc, gs, mc, gb, ob, gm, om, gf, gsec, of, osec,
    BB, MB, RAW, U, SQ, MO,
    X, C, BS, MS, PT, LB, XR, ZS, ZR, FS, NM,
    li, ss, sr,
    g_zs, g_zr, g_xs, g_xr, g_os, g_or,
    d_s, d_r,
    y_s, y_r, yo_s, yo_r,
    rx_s, rx_r, rz_s, rz_r,
    az_s, az_r, ax_s, ax_r, ad_s, ad_r,
    pm_s, pm_r, sq_s, sq_r,
):
    z, x, c, y = (lax.axis_index(a) for a in ("z", "x", "core", "tp"))
    other = 1 - c

    def zat(k):
        return lax.rem(z + k + ZN, ZN)

    def xat(k):
        return lax.rem(x + k + XN, XN)

    def yat(k):
        return lax.rem(y + k + YN, YN)

    dsts = (BS.at[c], X.at[c], C.at[c], MS.at[c], FS.at[0, c], FS.at[1, c])
    gates = (gb, bi, gc, gm, gf, gsec)
    outs = (ob, mc, gs, om, of, osec)

    def load(mine):
        for k in range(6):
            pltpu.make_async_copy(mine[k], dsts[k], li.at[k]).start()

    def ship(theirs):
        for k in range(6):
            remote(theirs[k], dsts[k], ss.at[k], sr.at[k], core=other).start()

    pl.when(c == 0)(lambda: load(gates))
    pl.when(c == 1)(lambda: load(outs))

    barrier = pltpu.get_barrier_semaphore()
    for k in (1, -1, 2, -2):
        pl.semaphore_signal(barrier, inc=1, device_id={"z": zat(k)}, device_id_type=MESH)
    for k in (1, -1):
        pl.semaphore_signal(barrier, inc=1, device_id={"x": xat(k)}, device_id_type=MESH)
        pl.semaphore_signal(barrier, inc=1, device_id={"tp": yat(k)}, device_id_type=MESH)
    pl.semaphore_signal(barrier, inc=1, device_id={"core": other}, device_id_type=MESH)

    at = lax.broadcasted_iota(jnp.int32, (low_rank, low_rank), 0)
    to = lax.broadcasted_iota(jnp.int32, (low_rank, low_rank), 1)
    source = ((to >> 3) & 3) * 128 + ((to >> 7) & 3) * 32 + ((to >> 5) & 3) * 8 + (to & 7)
    by_owner = jnp.where(at == source, 1.0, 0.0).astype(BF)

    pl.semaphore_wait(barrier, 9)

    pl.when(c == 0)(lambda: ship(outs))
    pl.when(c == 1)(lambda: ship(gates))

    def arrived(k):
        ref = dsts[k]
        pltpu.make_async_copy(gates[k], ref, li.at[k]).wait()
        remote(ref, ref, ss.at[k], sr.at[k], core=other).wait_recv()

    def gather(g, buf):
        zs, zr, xs, xr, os, orr = g_zs.at[g], g_zr.at[g], g_xs.at[g], g_xr.at[g], g_os.at[g], g_or.at[g]

        def got(ref, sem):
            remote(ref, ref, zs, sem, z=zat(1)).wait_recv()

        def zof(i):
            d = (i + 1) // 2
            return lax.rem(z + ZN + (1 - 2 * lax.rem(i, 2)) * d, ZN)

        def zsends(s):
            for sign, far in ((1, ZN // 2), (-1, ZN // 2 - 1)):
                src = buf.at[zat(-sign * 2 * s), x]
                for k in (2, 1):
                    if 2 * s + k <= far:
                        i = block_id(sign, 2 * s + k)
                        remote(src, src, zs, zr.at[(i - 1) // 2], z=zat(sign * k)).start()

        def zwait(k):
            got(buf.at[0:2, x] if k < 7 else buf.at[0, x], zr.at[k])

        def each(f, lo, hi):
            def body(i, _):
                f(i)
                return 0
            lax.fori_loop(lo, hi, body, 0)

        groups = ((0, 1), (1, 5), (5, 9), (9, 13), (13, 16))

        def forward(n):
            def one(i):
                ref = buf.at[zof(i), x]
                remote(ref, ref, xs, xr.at[n], x=xat(1)).start()
                remote(ref, ref, xs, xr.at[n], x=xat(-1)).start()
                if n == 4:
                    remote(ref, ref, os, orr, x=xat(2)).start()
            each(one, *groups[n])

        def relay(n):
            def one(i):
                zz = zof(i)
                a, b = buf.at[zz, xat(-1), pl.ds(0, 16)], buf.at[zz, xat(1), pl.ds(16, 16)]
                remote(a, a, os, orr, x=xat(1)).start()
                remote(b, b, os, orr, x=xat(-1)).start()
            lo, hi = groups[n]
            got(buf.at[0:2, 0] if n == 0 else buf.at[0:2], xr.at[n])
            each(one, lo, hi)

        def along_z(s):
            if s > 0:
                zwait(2 * s - 1)
            zsends(s)

        def along_x(n):
            if n > 0:
                zwait(2 * n - 2)
            if n == 4:
                zwait(7)
            forward(n)

        def opposite():
            got(buf.at[0:6, 0], xr.at[4])
            got(buf.at[0:4], orr)

        def finish():
            remote(buf.at[0:15, 0], buf.at[0:15, 0], zs, zr.at[0], z=zat(1)).wait_send()
            remote(buf.at[0:8], buf.at[0:8], xs, zr.at[0], z=zat(1)).wait_send()
            remote(buf.at[0:4], buf.at[0:4], os, zr.at[0], z=zat(1)).wait_send()

        return along_z, along_x, relay, opposite, finish

    Az, Ax, Ar, Ao, a_finish = gather(0, BB.at[c, 0])
    Bz, Bx, Br, Bo, b_finish = gather(1, BB.at[c, 1])
    Mz, Mx, Mr, Mo, m_finish = gather(2, MB.at[c])
    half = low_rank // 2

    arrived(0)
    ordered = jnp.dot(BS[...].reshape(32, low_rank), by_owner, preferred_element_type=F32).astype(BF)
    BB[c, 0, z, x] = ordered[:, :half]
    BB[c, 1, z, x] = ordered[:, half:]
    for s in range(4):
        Az(s)
        Ax(s)
        if s >= 2:
            Ar(s - 2)
        Bz(s)
        if s >= 1:
            Bx(s - 1)
    Ax(4)
    Ar(2)
    Bx(3)
    Br(0)
    arrived(3)
    MB[c, z, x] = MS[...].reshape(32, inner).astype(BF)
    Mz(0)
    Ar(3)
    Bx(4)
    Br(1)
    Br(2)
    Ao()
    arrived(1)

    W = low_rank // NC
    tokens = 512

    def y_copies(u):
        ref = PT.at[y, u]
        return [
            remote(ref, ref, y_s, y_r.at[0, u], tp=yat(1)),
            remote(ref, ref, y_s, y_r.at[1, u], tp=yat(-1)),
        ]

    def project(h):
        basis = BB[c, h].reshape(ZN * XN * 32, half)
        proj = jnp.dot(X[...].reshape(tokens, -1), basis, preferred_element_type=F32).T.astype(BF)
        for k in range(NC // 2):
            PT[y, h * (NC // 2) + k] = proj[k * W : (k + 1) * W]

    def send_projected(h):
        for k in range(NC // 2):
            for copy in y_copies(h * (NC // 2) + k):
                copy.start()

    def y_relays(u):
        left, right = PT.at[yat(-1), u], PT.at[yat(1), u]
        a, b = PT.at[yat(-1), u, pl.ds(0, W // 2)], PT.at[yat(1), u, pl.ds(W // 2, W // 2)]
        return (
            remote(left, left, y_s, y_r.at[0, u], tp=yat(1)),
            remote(right, right, y_s, y_r.at[1, u], tp=yat(-1)),
            remote(a, a, yo_s, yo_r.at[u], tp=yat(1)),
            remote(b, b, yo_s, yo_r.at[u], tp=yat(-1)),
        )

    def y_stage(u):
        l, r, a, b = y_relays(u)
        l.wait_recv()
        a.start()
        r.wait_recv()
        b.start()

    def rx_copies(u):
        return [
            remote(LB.at[u, xat(d)], XR.at[u, d - 1], rx_s, rx_r.at[u], x=xat(d))
            for d in (1, 2, 3)
        ]

    def low_stage(u):
        ref = PT.at[yat(2), u]
        remote(ref, ref, yo_s, yo_r.at[u], tp=yat(1)).wait_recv()

        def add(k, total):
            rows = pl.ds(pl.multiple_of(k * 256, 256), 256)
            for h in range(2):
                total += jnp.dot(
                    PT[k, u, :, h * 256 : (h + 1) * 256], C[h, rows], preferred_element_type=F32
                )
            return total

        total = lax.fori_loop(0, YN, add, jnp.zeros((W, inner), F32))
        LB[u] = total.reshape(XN, ZQ, OWN, inner).astype(BF)
        for copy in rx_copies(u):
            copy.start()

    def rz_copy(u, q):
        to = q * NC + u
        return remote(ZS.at[u, q], ZR.at[z], rz_s, rz_r, z=to)

    def rx_stage(u):
        total = LB[u, x].astype(F32)
        remote(XR.at[u], XR.at[u], rx_s, rx_r.at[u], x=xat(1)).wait_recv()
        for d in range(3):
            total += XR[u, d].astype(F32)
        ZS[u] = total.astype(BF)
        for q in range(ZQ):
            pl.when(z != q * NC + u)(lambda: rz_copy(u, q).start())

    zq = z // NC

    def az_copy(u, d):
        ref = RAW.at[c, u, x, zq]
        return remote(ref, ref, az_s, az_r.at[u], z=zat(d))

    def pm_copy():
        return remote(NM.at[other], MO.at[pl.ds(2 * c, 2)], pm_s, pm_r, core=other)

    def rz_stage(u):
        @pl.when(lax.rem(z, NC) == u)
        def _():
            def add(d, total):
                return total + ZR[zat(d)].astype(F32)

            remote(ZR.at[0:15], ZR.at[0:15], rz_s, rz_r, z=zat(1)).wait_recv()
            low = lax.fori_loop(1, ZN, add, ZS[u, zq].astype(F32))
            raws = []
            for h in range(2):
                part = low[4 * h : 4 * h + 4]
                first = 0.9 * FS[0, h] + 0.1 * part
                second = 0.95 * FS[1, h] + 0.05 * part * part
                NM[h, 0] = first
                NM[h, 1] = second
                raws.append(first / jnp.sqrt(second))
            RAW[c, u, x, zq] = jnp.concatenate(raws, axis=0).astype(BF)

            def send(d, _):
                az_copy(u, d).start()
                return 0

            lax.fori_loop(1, ZN, send, 0)
            pm_copy().start()
            MO[pl.ds(2 * c, 2)] = NM[c]

    def ax_copies(u):
        ref = RAW.at[c, u, x]
        return [
            remote(ref, ref, ax_s, ax_r.at[u], x=xat(d)) for d in (1, 2, 3)
        ]

    def az_stage(u):
        def landed(n):
            ref = RAW.at[c, u, x, pl.ds(0, n)]
            remote(ref, ref, az_s, az_r.at[u], z=zat(1)).wait_recv()

        pl.when(lax.rem(z, NC) == u)(lambda: landed(ZQ - 1))
        pl.when(lax.rem(z, NC) != u)(lambda: landed(ZQ))
        for copy in ax_copies(u):
            copy.start()

    def ad_copy(u):
        ref = RAW.at[c, u]
        return remote(ref, ref, ad_s, ad_r.at[u], core=other)

    def ax_stage(u):
        ref = RAW.at[c, u, pl.ds(0, 3)]
        remote(ref, ref, ax_s, ax_r.at[u], x=xat(1)).wait_recv()
        ad_copy(u).start()

    def ad_stage(u):
        ref = RAW.at[other, u]
        remote(ref, ref, ad_s, ad_r.at[u], core=other).wait_recv()

    project(0)
    send_projected(0)
    Br(3)
    Mz(1)
    whole = [
        remote(BB.at[c], BB.at[c], d_s.at[0], d_r.at[0], core=other),
        remote(MB.at[c], MB.at[c], d_s.at[1], d_r.at[1], core=other),
    ]
    Bo()
    project(1)
    y_stage(0)
    send_projected(1)
    whole[0].start()
    Mx(0)
    Mx(1)
    y_stage(1)
    Mz(2)
    Mx(2)
    for k in (2, 4, 5):
        arrived(k)
    low_stage(0)
    Mr(0)
    Mr(1)
    y_stage(2)
    Mz(3)
    Mx(3)
    y_stage(3)
    low_stage(1)
    rx_stage(0)
    Mr(2)
    low_stage(2)
    rx_stage(1)
    low_stage(3)
    Mx(4)
    rx_stage(2)
    rx_stage(3)
    Mr(3)
    for u in range(NC):
        rz_stage(u)
    az_stage(0)
    Mo()
    whole[1].start()
    for u in range(1, NC):
        az_stage(u)
    ax_stage(0)
    ax_stage(1)

    def begin(m):
        def some(t, _):
            zz, rows = pl.ds(t * 2, 2), pl.ds(pl.multiple_of(t * 256, 256), 256)
            U[m, rows] = jnp.dot(
                BB[m, 0, zz].reshape(256, half),
                RAW[m, 0 : NC // 2].reshape(half, inner),
                preferred_element_type=F32,
            )
            return 0

        lax.fori_loop(0, 8, some, 0)

    begin(c)
    ax_stage(2)
    ad_stage(0)
    ad_stage(1)
    remote(BB.at[other], BB.at[other], d_s.at[0], d_r.at[0], core=other).wait_recv()
    begin(other)

    def squares(m, u):
        r = RAW[m, u].reshape(W, inner).astype(F32)
        r = (r * r).reshape(W // 8, 8, inner).sum(axis=0)
        return sum(r[:, k * 128 : (k + 1) * 128] for k in range(inner // 128))

    total = jnp.zeros((8, 128), F32)
    for u in range(NC // 2):
        total += squares(0, u) + squares(1, u)
    ad_stage(2)
    total += squares(0, 2) + squares(1, 2)
    ax_stage(3)
    total += squares(c, 3)
    ad_stage(3)
    SQ[y] = total + squares(other, 3)

    def sq_copy(d):
        return remote(SQ.at[y], SQ.at[y], sq_s, sq_r, tp=yat(d))

    for d in (1, 2, 3):
        sq_copy(d).start()
    remote(SQ.at[0:3], SQ.at[0:3], sq_s, sq_r, tp=yat(1)).wait_recv()

    remote(MB.at[other], MB.at[other], d_s.at[1], d_r.at[1], core=other).wait_recv()
    remote(NM.at[c], NM.at[c], pm_s, pm_r, core=other).wait_recv()

    for k in range(6):
        remote(dsts[k], dsts[k], ss.at[k], sr.at[k], core=other).wait_send()
    a_finish()
    b_finish()
    m_finish()
    for copy in whole:
        copy.wait_send()
    for ref, sem in ((PT.at[0:2], y_s), (PT.at[0], yo_s), (XR, rx_s), (XR, ax_s), (LB, ad_s)):
        remote(ref, ref, sem, y_r.at[0, 0], tp=yat(1)).wait_send()
    fifteen = ZR.at[0:15]
    remote(fifteen, fifteen, rz_s, rz_r, z=zat(1)).wait_send()
    remote(fifteen, fifteen, az_s, rz_r, z=zat(1)).wait_send()
    pm_copy().wait_send()
    remote(SQ.at[0:3], SQ.at[0:3], sq_s, sq_r, tp=yat(1)).wait_send()


def finish(
    low_rank, inner,
    BB, MB, RAW, U, SQ, MO, gm, om,
    gm_out, om_out, gcopy, ocopy, gf_out, gs_out, of_out, os_out,
    GO, OO, out_s,
):
    z, x, c = (lax.axis_index(a) for a in ("z", "x", "core"))
    half = low_rank // 2
    own_rows = pl.ds(pl.multiple_of(c * 16, 16), 16)
    total = jnp.sum(SQ[0] + SQ[1] + SQ[2] + SQ[3])
    scale = 0.25 * lax.rsqrt(
        jnp.full((1, inner), total, F32) / (2.0 * low_rank * inner * YN) + 1e-06
    )
    TILE = 256

    def gate_out(t):
        rows = pl.ds(pl.multiple_of(t * TILE, TILE), TILE)
        return pltpu.make_async_copy(GO.at[rows], gcopy.at[rows], out_s.at[0, t])

    def out_out(t):
        rows = pl.ds(pl.multiple_of(t * TILE, TILE), TILE)
        return pltpu.make_async_copy(OO.at[:, rows], ocopy.at[:, rows], out_s.at[1, t])

    raws = [RAW[m, NC // 2 :].reshape(half, inner) for m in range(2)]

    def update(m, basis, rows):
        return scale * (U[m, rows] + jnp.dot(basis, raws[m], preferred_element_type=F32))

    def tile(t, _):
        zz = pl.ds(t * 2, 2)
        rows = pl.ds(pl.multiple_of(t * TILE, TILE), TILE)
        up = update(0, BB[0, 1, zz].reshape(TILE, half), rows)
        GO[rows] = (MB[0, zz].reshape(TILE, inner).astype(F32) - up).astype(BF)
        gate_out(t).start()
        up = update(1, BB[1, 1, zz].reshape(TILE, half), rows)
        OO[:, rows] = (MB[1, zz].reshape(TILE, inner).astype(F32) - up).T.astype(BF)
        out_out(t).start()
        return 0

    lax.fori_loop(0, 8, tile, 0)
    mine = pl.ds(pl.multiple_of((z * XN + x) * 32 + c * 16, 16), 16)
    gm_out[...] = gm[...] - update(0, BB[0, 1, z, x, own_rows], mine)
    om_out[...] = om[...] - update(1, BB[1, 1, z, x, own_rows], mine)
    for k, ref in enumerate((gf_out, gs_out, of_out, os_out)):
        ref[...] = MO[k]

    def done(t, _):
        gate_out(t).wait()
        out_out(t).wait()
        return 0

    lax.fori_loop(0, 8, done, 0)


def on_device(
    block_input, gate_cotangent, gated_state, mixer_cotangent, gate_basis, out_basis,
    gate_master, out_master, gate_first, gate_second, out_first, out_second,
):
    low_rank = gate_basis.shape[1]
    inner = gate_first.shape[1]
    rows = gate_basis.shape[0]

    out_t = out_master.T
    D = pltpu.SemaphoreType.DMA
    V = pltpu.VMEM
    full = rows * ZN * XN * 2
    W = low_rank // NC
    held = (
        jax.ShapeDtypeStruct((2, 2, ZN, XN, 32, low_rank // 2), BF),
        jax.ShapeDtypeStruct((2, ZN, XN, 32, inner), BF),
        jax.ShapeDtypeStruct((2, NC, XN, ZQ, OWN, inner), BF),
        jax.ShapeDtypeStruct((2, full, inner), F32),
        jax.ShapeDtypeStruct((YN, 8, 128), F32),
        jax.ShapeDtypeStruct((4, *gate_first.shape), F32),
    )
    vmem = pl.BlockSpec(memory_space=pltpu.VMEM)
    hbm = pl.BlockSpec(memory_space=pltpu.HBM)
    held = pl.pallas_call(
        functools.partial(kernel, low_rank, inner),
        out_shape=held,
        in_specs=[hbm] * 12,
        out_specs=[vmem] * 6,
        scratch_shapes=[
            V((2, 256, full), BF),
            V((2, 1024, inner), BF),
            V((2, rows, low_rank), BF),
            V((2, rows, inner), F32),
            V((YN, NC, W, 512), BF),
            V((NC, XN, ZQ, OWN, inner), BF),
            V((NC, 3, ZQ, OWN, inner), BF),
            V((NC, ZQ, OWN, inner), BF),
            V((ZN, OWN, inner), BF),
            V((2, 2, 4, inner), F32),
            V((2, 2, 4, inner), F32),
            D((6,)), D((6,)), D((6,)),
            D((3,)), D((3, NID // 2)), D((3,)), D((3, 5)), D((3,)), D((3,)),
            D((2,)), D((2,)),
            D, D((2, NC)), D, D((NC,)),
            D, D((NC,)), D, D,
            D, D((NC,)), D, D((NC,)), D, D((NC,)),
            D, D, D, D,
        ],
        compiler_params=pltpu.CompilerParams(
            collective_id=0, has_side_effects=True, vmem_limit_bytes=LIMIT1
        ),
        name="moment_update",
    )(
        *(pltpu.with_memory_space_constraint(a, pltpu.HBM) for a in (
            block_input, gate_cotangent, gated_state, mixer_cotangent, gate_basis, out_basis,
            gate_master, out_t, gate_first, gate_second, out_first, out_second,
        ))
    )
    outs = (
        jax.ShapeDtypeStruct((rows, inner), F32),
        jax.ShapeDtypeStruct((rows, inner), F32),
        jax.ShapeDtypeStruct((full, inner), BF),
        jax.ShapeDtypeStruct((inner, full), BF),
    ) + (jax.ShapeDtypeStruct(gate_first.shape, F32),) * 4
    res = pl.pallas_call(
        functools.partial(finish, low_rank, inner),
        out_shape=outs,
        in_specs=[vmem] * 8,
        out_specs=[vmem, vmem, hbm, hbm, vmem, vmem, vmem, vmem],
        scratch_shapes=[V((full, inner), BF), V((inner, full), BF), D((2, 8))],
        compiler_params=pltpu.CompilerParams(vmem_limit_bytes=LIMIT2),
        name="apply_step",
    )(*held, gate_master, out_t)
    return (res[0], res[1].T, *res[2:])


def solution(mesh):
    finer = Mesh(mesh.devices.reshape(ZN, XN, 2, mesh.shape["tp"]), FS_TP)
    in_specs = (
        P(FS_TP, None), P(FSN, "tp"), P(FSN, "tp"), P(FS_TP, None), P(FSN, None), P(FSN, None),
        P(FSN, "tp"), P("tp", FSN), P(FSN, "tp"), P(FSN, "tp"), P(FSN, "tp"), P(FSN, "tp"),
    )
    out_specs = (
        P(FSN, "tp"), P("tp", FSN), P(None, "tp"), P("tp", None),
        P(FSN, "tp"), P(FSN, "tp"), P(FSN, "tp"), P(FSN, "tp"),
    )
    return jax.shard_map(
        on_device, mesh=finer, in_specs=in_specs, out_specs=out_specs, check_vma=False
    )
```

```python
import functools

import jax
import jax.numpy as jnp
from jax import lax
from jax.experimental import pallas as pl
from jax.experimental.pallas import tpu as pltpu
from jax.sharding import Mesh
from jax.sharding import PartitionSpec as P

MESH = pl.DeviceIdType.MESH
BF = jnp.bfloat16
F32 = jnp.float32
ZN, XN, YN = 16, 4, 4
FSN = ("z", "x", "core")
FS_TP = ("z", "x", "core", "tp")
NC = 4
ZQ = ZN // NC
OWN = 8
LIMIT1 = 30 * 1024 * 1024
LIMIT2 = 8 * 1024 * 1024
NID = ZN


def block_id(sign, dist):
    return 2 * dist - 1 if sign > 0 else 2 * dist


def remote(src, dst, send, recv, **to):
    return pltpu.make_async_remote_copy(
        src_ref=src, dst_ref=dst, send_sem=send, recv_sem=recv, device_id=to, device_id_type=MESH
    )


def kernel(
    low_rank, inner,
    bi, gc, gs, mc, gb, ob, gm, om, gf, gsec, of, osec,
    MB, U, V, N, OR, SQ, MO,
    BB, RAW, BT, RT, LP, X, C, BS, MS, PT, LB, XR, ZS, ZR, FS, NM,
    li, ss, sr,
    g_zs, g_zr, g_xs, g_xr, g_os, g_or,
    d_s, d_r,
    y_s, y_r, yo_s, yo_r,
    rx_s, rx_r, rz_s, rz_r,
    az_s, az_r, ax_s, ax_r, ad_s, ad_r,
    pm_s, pm_r, sq_s, sq_r,
):
    z, x, c, y = (lax.axis_index(a) for a in ("z", "x", "core", "tp"))
    other = 1 - c

    def zat(k):
        return lax.rem(z + k + ZN, ZN)

    def xat(k):
        return lax.rem(x + k + XN, XN)

    def yat(k):
        return lax.rem(y + k + YN, YN)

    dsts = (BS.at[c], X.at[c], C.at[c], MS.at[c], FS.at[0, c], FS.at[1, c])
    gates = (gb, bi, gc, gm, gf, gsec)
    outs = (ob, mc, gs, om, of, osec)

    def load(mine):
        for k in range(6):
            pltpu.make_async_copy(mine[k], dsts[k], li.at[k]).start()

    def ship(theirs):
        for k in range(6):
            remote(theirs[k], dsts[k], ss.at[k], sr.at[k], core=other).start()

    pl.when(c == 0)(lambda: load(gates))
    pl.when(c == 1)(lambda: load(outs))

    barrier = pltpu.get_barrier_semaphore()
    for k in (1, -1, 2, -2):
        pl.semaphore_signal(barrier, inc=1, device_id={"z": zat(k)}, device_id_type=MESH)
    for k in (1, -1):
        pl.semaphore_signal(barrier, inc=1, device_id={"x": xat(k)}, device_id_type=MESH)
        pl.semaphore_signal(barrier, inc=1, device_id={"tp": yat(k)}, device_id_type=MESH)
    pl.semaphore_signal(barrier, inc=1, device_id={"core": other}, device_id_type=MESH)

    at = lax.broadcasted_iota(jnp.int32, (low_rank, low_rank), 0)
    to = lax.broadcasted_iota(jnp.int32, (low_rank, low_rank), 1)
    source = ((to >> 3) & 3) * 128 + ((to >> 7) & 3) * 32 + ((to >> 5) & 3) * 8 + (to & 7)
    by_owner = jnp.where(at == source, 1.0, 0.0).astype(BF)

    pl.semaphore_wait(barrier, 9)

    pl.when(c == 0)(lambda: ship(outs))
    pl.when(c == 1)(lambda: ship(gates))

    def arrived(k):
        ref = dsts[k]
        pltpu.make_async_copy(gates[k], ref, li.at[k]).wait()
        remote(ref, ref, ss.at[k], sr.at[k], core=other).wait_recv()

    def gather(g, buf):
        zs, zr, xs, xr, os, orr = g_zs.at[g], g_zr.at[g], g_xs.at[g], g_xr.at[g], g_os.at[g], g_or.at[g]

        def got(ref, sem):
            remote(ref, ref, zs, sem, z=zat(1)).wait_recv()

        def zof(i):
            d = (i + 1) // 2
            return lax.rem(z + ZN + (1 - 2 * lax.rem(i, 2)) * d, ZN)

        def zsends(s):
            for sign, far in ((1, ZN // 2), (-1, ZN // 2 - 1)):
                src = buf.at[zat(-sign * 2 * s), x]
                for k in (2, 1):
                    if 2 * s + k <= far:
                        i = block_id(sign, 2 * s + k)
                        remote(src, src, zs, zr.at[(i - 1) // 2], z=zat(sign * k)).start()

        def zwait(k):
            got(buf.at[0:2, x] if k < 7 else buf.at[0, x], zr.at[k])

        def each(f, lo, hi):
            def body(i, _):
                f(i)
                return 0
            lax.fori_loop(lo, hi, body, 0)

        groups = ((0, 1), (1, 5), (5, 9), (9, 13), (13, 16))

        def forward(n):
            def one(i):
                ref = buf.at[zof(i), x]
                remote(ref, ref, xs, xr.at[n], x=xat(1)).start()
                remote(ref, ref, xs, xr.at[n], x=xat(-1)).start()
                if n == 4:
                    remote(ref, ref, os, orr, x=xat(2)).start()
            each(one, *groups[n])

        def relay(n):
            def one(i):
                zz = zof(i)
                a, b = buf.at[zz, xat(-1), pl.ds(0, 16)], buf.at[zz, xat(1), pl.ds(16, 16)]
                remote(a, a, os, orr, x=xat(1)).start()
                remote(b, b, os, orr, x=xat(-1)).start()
            lo, hi = groups[n]
            got(buf.at[0:2, 0] if n == 0 else buf.at[0:2], xr.at[n])
            each(one, lo, hi)

        def along_z(s):
            if s > 0:
                zwait(2 * s - 1)
            zsends(s)

        def along_x(n):
            if n > 0:
                zwait(2 * n - 2)
            if n == 4:
                zwait(7)
            forward(n)

        def opposite():
            got(buf.at[0:6, 0], xr.at[4])
            got(buf.at[0:4], orr)

        def finish():
            remote(buf.at[0:15, 0], buf.at[0:15, 0], zs, zr.at[0], z=zat(1)).wait_send()
            remote(buf.at[0:8], buf.at[0:8], xs, zr.at[0], z=zat(1)).wait_send()
            remote(buf.at[0:4], buf.at[0:4], os, zr.at[0], z=zat(1)).wait_send()

        return along_z, along_x, relay, opposite, finish

    Az, Ax, Ar, Ao, a_finish = gather(0, BB.at[c, 0])
    Bz, Bx, Br, Bo, b_finish = gather(1, BB.at[c, 1])
    Mz, Mx, Mr, Mo, m_finish = gather(2, MB.at[c])
    half = low_rank // 2

    arrived(0)
    ordered = jnp.dot(BS[...].reshape(32, low_rank), by_owner, preferred_element_type=F32).astype(BF)
    BB[c, 0, z, x] = ordered[:, :half]
    BB[c, 1, z, x] = ordered[:, half:]
    for s in range(4):
        Az(s)
        Ax(s)
        if s >= 2:
            Ar(s - 2)
        Bz(s)
        if s >= 1:
            Bx(s - 1)
    Ax(4)
    Ar(2)
    Ar(3)
    Bx(3)
    Br(0)
    arrived(3)
    MB[c, z, x] = MS[...].reshape(32, inner).astype(BF)
    Mz(0)
    Bx(4)
    Br(1)
    Br(2)
    Ao()
    arrived(1)

    W = low_rank // NC
    tokens = 512

    def y_copies(u):
        ref = PT.at[y, u]
        return [
            remote(ref, ref, y_s, y_r.at[0, u], tp=yat(1)),
            remote(ref, ref, y_s, y_r.at[1, u], tp=yat(-1)),
        ]

    def project(h):
        basis = BB[c, h].reshape(ZN * XN * 32, half)
        proj = jnp.dot(X[...].reshape(tokens, -1), basis, preferred_element_type=F32).T.astype(BF)
        for k in range(NC // 2):
            PT[y, h * (NC // 2) + k] = proj[k * W : (k + 1) * W]

    def send_projected(u):
        for copy in y_copies(u):
            copy.start()

    def y_relays(u):
        left, right = PT.at[yat(-1), u], PT.at[yat(1), u]
        a, b = PT.at[yat(-1), u, pl.ds(0, W // 2)], PT.at[yat(1), u, pl.ds(W // 2, W // 2)]
        return (
            remote(left, left, y_s, y_r.at[0, u], tp=yat(1)),
            remote(right, right, y_s, y_r.at[1, u], tp=yat(-1)),
            remote(a, a, yo_s, yo_r.at[u], tp=yat(1)),
            remote(b, b, yo_s, yo_r.at[u], tp=yat(-1)),
        )

    def y_stage(u):
        l, r, a, b = y_relays(u)
        l.wait_recv()
        a.start()
        r.wait_recv()
        b.start()

    def rx_copies(u):
        return [
            remote(LB.at[u, xat(d)], XR.at[u, d - 1], rx_s, rx_r.at[u], x=xat(d))
            for d in (2, 3, 1)
        ]

    def term(k, u):
        rows = pl.ds(pl.multiple_of(k * 256, 256), 256)
        return sum(
            jnp.dot(PT[k, u, :, h * 256 : (h + 1) * 256], C[h, rows], preferred_element_type=F32)
            for h in range(2)
        )

    def near_stage(u):
        LP[...] = term(y, u) + term(yat(1), u) + term(yat(-1), u)

    def low_stage(u):
        ref = PT.at[yat(2), u]
        remote(ref, ref, yo_s, yo_r.at[u], tp=yat(1)).wait_recv()
        total = LP[...] + term(yat(2), u)
        LB[u] = total.reshape(XN, ZQ, OWN, inner).astype(BF)
        for copy in rx_copies(u):
            copy.start()

    def rz_copy(u, q):
        to = q * NC + u
        return remote(ZS.at[u, q], ZR.at[z], rz_s, rz_r, z=to)

    def rx_stage(u):
        total = LB[u, x].astype(F32)
        remote(XR.at[u], XR.at[u], rx_s, rx_r.at[u], x=xat(1)).wait_recv()
        for d in range(3):
            total += XR[u, d].astype(F32)
        ZS[u] = total.astype(BF)
        for q in range(ZQ):
            pl.when(z != q * NC + u)(lambda: rz_copy(u, q).start())

    zq = z // NC

    def az_copy(u, d):
        ref = RAW.at[c, u, x, zq]
        return remote(ref, ref, az_s, az_r.at[u], z=zat(d))

    def pm_copy():
        return remote(NM.at[other], MO.at[pl.ds(2 * c, 2)], pm_s, pm_r, core=other)

    def rz_stage(u):
        @pl.when(lax.rem(z, NC) == u)
        def _():
            def add(d, total):
                return total + ZR[zat(d)].astype(F32)

            remote(ZR.at[0:15], ZR.at[0:15], rz_s, rz_r, z=zat(1)).wait_recv()
            low = lax.fori_loop(1, ZN, add, ZS[u, zq].astype(F32))
            raws = []
            for h in range(2):
                part = low[4 * h : 4 * h + 4]
                first = 0.9 * FS[0, h] + 0.1 * part
                second = 0.95 * FS[1, h] + 0.05 * part * part
                NM[h, 0] = first
                NM[h, 1] = second
                raws.append(first / jnp.sqrt(second))
            RAW[c, u, x, zq] = jnp.concatenate(raws, axis=0).astype(BF)

            def send(k, _):
                az_copy(u, ZN // 2 + (k + 1) // 2 * (1 - 2 * lax.rem(k, 2))).start()
                return 0

            lax.fori_loop(0, ZN - 1, send, 0)
            pm_copy().start()
            MO[pl.ds(2 * c, 2)] = NM[c]

    def ax_copies(u):
        ref = RAW.at[c, u, x]
        return [
            remote(ref, ref, ax_s, ax_r.at[u], x=xat(d)) for d in (2, 3, 1)
        ]

    def az_stage(u):
        def landed(n):
            ref = RAW.at[c, u, x, pl.ds(0, n)]
            remote(ref, ref, az_s, az_r.at[u], z=zat(1)).wait_recv()

        pl.when(lax.rem(z, NC) == u)(lambda: landed(ZQ - 1))
        pl.when(lax.rem(z, NC) != u)(lambda: landed(ZQ))
        for copy in ax_copies(u):
            copy.start()

    def ad_copy(u):
        ref = RAW.at[c, u]
        return remote(ref, ref, ad_s, ad_r.at[u], core=other)

    def ax_stage(u):
        ref = RAW.at[c, u, pl.ds(0, 3)]
        remote(ref, ref, ax_s, ax_r.at[u], x=xat(1)).wait_recv()
        ad_copy(u).start()

    def ad_stage(u):
        ref = RAW.at[other, u]
        remote(ref, ref, ad_s, ad_r.at[u], core=other).wait_recv()

    project(0)
    send_projected(0)
    send_projected(1)
    Br(3)
    Mz(1)
    Mx(0)
    Mx(1)
    whole = [
        remote(BB.at[c], BB.at[c], d_s.at[0], d_r.at[0], core=other),
        remote(MB.at[c], MB.at[c], d_s.at[1], d_r.at[1], core=other),
    ]
    Bo()
    project(1)
    Mz(2)
    Mx(2)
    y_stage(0)
    send_projected(2)
    whole[0].start()
    Mr(0)
    y_stage(1)
    send_projected(3)
    Mr(1)
    Mz(3)
    Mx(3)
    for k in (2, 4, 5):
        arrived(k)
    near_stage(0)
    low_stage(0)
    near_stage(1)
    y_stage(2)
    Mr(2)
    low_stage(1)
    near_stage(2)
    y_stage(3)
    rx_stage(0)
    low_stage(2)
    near_stage(3)
    Mx(4)
    rx_stage(1)
    low_stage(3)
    Mr(3)
    rx_stage(2)
    rx_stage(3)
    for u in range(NC):
        rz_stage(u)
    Mo()
    whole[1].start()
    remote(BB.at[other], BB.at[other], d_s.at[0], d_r.at[0], core=other).wait_recv()

    def turn_basis(t, _):
        rows = pl.ds(pl.multiple_of(t * 256, 256), 256)
        for h in range(2):
            BT[h, :, rows] = BB[1, h, pl.ds(t * 2, 2)].reshape(256, half).T
        return 0

    lax.fori_loop(0, 8, turn_basis, 0)
    az_stage(0)
    az_stage(1)
    landed = remote(MB.at[other], MB.at[other], d_s.at[1], d_r.at[1], core=other)
    pl.when(c == 0)(landed.wait_recv)

    def turn(t, _):
        rows = pl.ds(pl.multiple_of(t * 256, 256), 256)
        N[:, rows] = MB[1, pl.ds(t * 2, 2)].reshape(256, inner).T
        return 0

    lax.fori_loop(0, 8, turn, 0)
    az_stage(2)
    ax_stage(0)
    az_stage(3)
    ax_stage(1)

    def raw_half(m, h):
        return RAW[m, h * (NC // 2) : (h + 1) * (NC // 2)].reshape(half, inner)

    def gate_half(h):
        def some(t, _):
            zz, rows = pl.ds(t * 8, 8), pl.ds(pl.multiple_of(t * 1024, 1024), 1024)
            part = jnp.dot(
                BB[0, h, zz].reshape(1024, half), raw_half(0, h), preferred_element_type=F32
            )
            U[rows] = part if h == 0 else U[rows] + part
            return 0

        lax.fori_loop(0, 2, some, 0)

    def out_half(h):
        RT[...] = raw_half(1, h).T

        def some(t, _):
            rows = pl.ds(pl.multiple_of(t * 1024, 1024), 1024)
            part = jnp.dot(RT[...], BT[h, :, rows], preferred_element_type=F32)
            V[:, rows] = part if h == 0 else V[:, rows] + part
            return 0

        lax.fori_loop(0, 2, some, 0)

    pl.when(c == 0)(lambda: gate_half(0))
    pl.when(c == 1)(lambda: out_half(0))
    ax_stage(2)
    ad_stage(0)
    ad_stage(1)
    pl.when(c == 0)(lambda: out_half(0))
    pl.when(c == 1)(lambda: gate_half(0))

    def squares(m, u):
        r = RAW[m, u].reshape(W, inner).astype(F32)
        r = (r * r).reshape(W // 8, 8, inner).sum(axis=0)
        return sum(r[:, k * 128 : (k + 1) * 128] for k in range(inner // 128))

    total = jnp.zeros((8, 128), F32)
    for u in range(NC // 2):
        total += squares(0, u) + squares(1, u)
    ad_stage(2)
    total += squares(0, 2) + squares(1, 2)
    ax_stage(3)
    total += squares(c, 3)
    ad_stage(3)
    SQ[y] = total + squares(other, 3)

    def sq_copy(d):
        return remote(SQ.at[y], SQ.at[y], sq_s, sq_r, tp=yat(d))

    for d in (1, 2, 3):
        sq_copy(d).start()

    gate_half(1)
    out_half(1)
    own_rows = pl.ds(pl.multiple_of(c * 16, 16), 16)
    OR[...] = sum(
        jnp.dot(BB[1, h, z, x, own_rows], raw_half(1, h), preferred_element_type=F32)
        for h in range(2)
    )
    remote(SQ.at[0:3], SQ.at[0:3], sq_s, sq_r, tp=yat(1)).wait_recv()

    pl.when(c == 1)(landed.wait_recv)
    remote(NM.at[c], NM.at[c], pm_s, pm_r, core=other).wait_recv()

    for k in range(6):
        remote(dsts[k], dsts[k], ss.at[k], sr.at[k], core=other).wait_send()
    a_finish()
    b_finish()
    m_finish()
    for copy in whole:
        copy.wait_send()
    for ref, sem in ((PT.at[0:2], y_s), (PT.at[0], yo_s), (XR, rx_s), (XR, ax_s), (LB, ad_s)):
        remote(ref, ref, sem, y_r.at[0, 0], tp=yat(1)).wait_send()
    fifteen = ZR.at[0:15]
    remote(fifteen, fifteen, rz_s, rz_r, z=zat(1)).wait_send()
    remote(fifteen, fifteen, az_s, rz_r, z=zat(1)).wait_send()
    pm_copy().wait_send()
    remote(SQ.at[0:3], SQ.at[0:3], sq_s, sq_r, tp=yat(1)).wait_send()


def finish(
    low_rank, inner,
    MB, U, V, N, OR, SQ, MO, gm, om,
    gm_out, om_out, gcopy, ocopy, gf_out, gs_out, of_out, os_out,
    GO, OO, GMO, OMO, out_s, few_s,
):
    z, x, c = (lax.axis_index(a) for a in ("z", "x", "core"))
    total = jnp.sum(SQ[0] + SQ[1] + SQ[2] + SQ[3])
    full = GO.shape[0]
    few = [
        pltpu.make_async_copy(MO.at[k], ref, few_s.at[k])
        for k, ref in enumerate((gf_out, gs_out, of_out, os_out))
    ]
    for copy in few:
        copy.start()
    scale_t = 0.25 * lax.rsqrt(
        jnp.full((1, full), total, F32) / (2.0 * low_rank * inner * YN) + 1e-06
    )
    scale = scale_t[:, :inner]
    TILE = 256

    def gate_out(t):
        rows = pl.ds(pl.multiple_of(t * TILE, TILE), TILE)
        return pltpu.make_async_copy(GO.at[rows], gcopy.at[rows], out_s.at[0, t])

    def out_out(t):
        rows = pl.ds(pl.multiple_of(t * 64, 64), 64)
        return pltpu.make_async_copy(OO.at[rows], ocopy.at[rows], out_s.at[1, t])

    def tile(t, _):
        zz = pl.ds(t * 2, 2)
        rows = pl.ds(pl.multiple_of(t * TILE, TILE), TILE)
        GO[rows] = (MB[0, zz].reshape(TILE, inner).astype(F32) - scale * U[rows]).astype(BF)
        gate_out(t).start()
        rows = pl.ds(pl.multiple_of(t * 64, 64), 64)
        OO[rows] = (N[rows].astype(F32) - scale_t * V[rows]).astype(BF)
        out_out(t).start()
        return 0

    mine = pl.ds(pl.multiple_of((z * XN + x) * 32 + c * 16, 16), 16)
    GMO[...] = gm[...] - scale * U[mine]
    OMO[...] = om[...] - scale * OR[...]
    few += [
        pltpu.make_async_copy(GMO, gm_out, few_s.at[4]),
        pltpu.make_async_copy(OMO, om_out, few_s.at[5]),
    ]
    for copy in few[4:]:
        copy.start()
    lax.fori_loop(0, 8, tile, 0)
    mine = pl.ds(pl.multiple_of((z * XN + x) * 32 + c * 16, 16), 16)
    def done(t, _):
        gate_out(t).wait()
        out_out(t).wait()
        return 0

    lax.fori_loop(0, 8, done, 0)
    for copy in few:
        copy.wait()


def on_device(
    block_input, gate_cotangent, gated_state, mixer_cotangent, gate_basis, out_basis,
    gate_master, out_master, gate_first, gate_second, out_first, out_second,
):
    low_rank = gate_basis.shape[1]
    inner = gate_first.shape[1]
    rows = gate_basis.shape[0]

    out_t = out_master.T
    D = pltpu.SemaphoreType.DMA
    vm = pltpu.VMEM
    full = rows * ZN * XN * 2
    W = low_rank // NC
    held = (
        jax.ShapeDtypeStruct((2, ZN, XN, 32, inner), BF),
        jax.ShapeDtypeStruct((full, inner), F32),
        jax.ShapeDtypeStruct((inner, full), F32),
        jax.ShapeDtypeStruct((inner, full), BF),
        jax.ShapeDtypeStruct((rows, inner), F32),
        jax.ShapeDtypeStruct((YN, 8, 128), F32),
        jax.ShapeDtypeStruct((4, *gate_first.shape), F32),
    )
    vmem = pl.BlockSpec(memory_space=pltpu.VMEM)
    hbm = pl.BlockSpec(memory_space=pltpu.HBM)
    held = pl.pallas_call(
        functools.partial(kernel, low_rank, inner),
        out_shape=held,
        in_specs=[hbm] * 12,
        out_specs=[vmem] * 7,
        scratch_shapes=[
            vm((2, 2, ZN, XN, 32, low_rank // 2), BF),
            vm((2, NC, XN, ZQ, OWN, inner), BF),
            vm((2, low_rank // 2, full), BF),
            vm((inner, low_rank // 2), BF),
            vm((W, inner), F32),
            vm((2, 256, full), BF),
            vm((2, 1024, inner), BF),
            vm((2, rows, low_rank), BF),
            vm((2, rows, inner), F32),
            vm((YN, NC, W, 512), BF),
            vm((NC, XN, ZQ, OWN, inner), BF),
            vm((NC, 3, ZQ, OWN, inner), BF),
            vm((NC, ZQ, OWN, inner), BF),
            vm((ZN, OWN, inner), BF),
            vm((2, 2, 4, inner), F32),
            vm((2, 2, 4, inner), F32),
            D((6,)), D((6,)), D((6,)),
            D((3,)), D((3, NID // 2)), D((3,)), D((3, 5)), D((3,)), D((3,)),
            D((2,)), D((2,)),
            D, D((2, NC)), D, D((NC,)),
            D, D((NC,)), D, D,
            D, D((NC,)), D, D((NC,)), D, D((NC,)),
            D, D, D, D,
        ],
        compiler_params=pltpu.CompilerParams(
            collective_id=0, has_side_effects=True, vmem_limit_bytes=LIMIT1
        ),
        name="moment_update",
    )(
        *(pltpu.with_memory_space_constraint(a, pltpu.HBM) for a in (
            block_input, gate_cotangent, gated_state, mixer_cotangent, gate_basis, out_basis,
            gate_master, out_t, gate_first, gate_second, out_first, out_second,
        ))
    )
    outs = (
        jax.ShapeDtypeStruct((rows, inner), F32),
        jax.ShapeDtypeStruct((rows, inner), F32),
        jax.ShapeDtypeStruct((full, inner), BF),
        jax.ShapeDtypeStruct((inner, full), BF),
    ) + (jax.ShapeDtypeStruct(gate_first.shape, F32),) * 4
    res = pl.pallas_call(
        functools.partial(finish, low_rank, inner),
        out_shape=outs,
        in_specs=[vmem] * 9,
        out_specs=[hbm] * 8,
        scratch_shapes=[
            vm((full, inner), BF), vm((inner, full), BF), vm((rows, inner), F32), vm((rows, inner), F32),
            D((2, 8)), D((6,)),
        ],
        compiler_params=pltpu.CompilerParams(vmem_limit_bytes=LIMIT2),
        name="apply_step",
    )(*held, gate_master, out_t)
    return (res[0], res[1].T, *res[2:])


def solution(mesh):
    finer = Mesh(mesh.devices.reshape(ZN, XN, 2, mesh.shape["tp"]), FS_TP)
    in_specs = (
        P(FS_TP, None), P(FSN, "tp"), P(FSN, "tp"), P(FS_TP, None), P(FSN, None), P(FSN, None),
        P(FSN, "tp"), P("tp", FSN), P(FSN, "tp"), P(FSN, "tp"), P(FSN, "tp"), P(FSN, "tp"),
    )
    out_specs = (
        P(FSN, "tp"), P("tp", FSN), P(None, "tp"), P("tp", None),
        P(FSN, "tp"), P(FSN, "tp"), P(FSN, "tp"), P(FSN, "tp"),
    )
    return jax.shard_map(
        on_device, mesh=finer, in_specs=in_specs, out_specs=out_specs, check_vma=False
    )
```

```python
import functools

import jax
import jax.numpy as jnp
from jax import lax
from jax.experimental import pallas as pl
from jax.experimental.pallas import tpu as pltpu
from jax.sharding import Mesh
from jax.sharding import PartitionSpec as P

MESH = pl.DeviceIdType.MESH
BF = jnp.bfloat16
F32 = jnp.float32
ZN, XN, YN = 16, 4, 4
FSN = ("z", "x", "core")
FS_TP = ("z", "x", "core", "tp")
NC = 4
ZQ = ZN // NC
OWN = 8
LIMIT1 = 30 * 1024 * 1024
LIMIT2 = 8 * 1024 * 1024
NID = ZN


def block_id(sign, dist):
    return 2 * dist - 1 if sign > 0 else 2 * dist


def remote(src, dst, send, recv, **to):
    return pltpu.make_async_remote_copy(
        src_ref=src, dst_ref=dst, send_sem=send, recv_sem=recv, device_id=to, device_id_type=MESH
    )


def kernel(
    low_rank, inner,
    bi, gc, gs, mc, gb, ob, gm, om, gf, gsec, of, osec,
    MB, U, V, N, OR, SQ, MO,
    BB, RAW, BT, RT, LP, X, C, BS, MS, PT, LB, XR, ZS, ZR, FS, NM,
    li, ss, sr,
    g_zs, g_zr, g_xs, g_xr, g_os, g_or,
    d_s, d_r,
    y_s, y_r, yo_s, yo_r,
    rx_s, rx_r, rz_s, rz_r,
    az_s, az_r, ax_s, ax_r, ad_s, ad_r,
    pm_s, pm_r, sq_s, sq_r,
):
    z, x, c, y = (lax.axis_index(a) for a in ("z", "x", "core", "tp"))
    other = 1 - c

    def zat(k):
        return lax.rem(z + k + ZN, ZN)

    def xat(k):
        return lax.rem(x + k + XN, XN)

    def yat(k):
        return lax.rem(y + k + YN, YN)

    dsts = (BS.at[c], X.at[c], C.at[c], MS.at[c], FS.at[0, c], FS.at[1, c])
    gates = (gb, bi, gc, gm, gf, gsec)
    outs = (ob, mc, gs, om, of, osec)

    def load(mine):
        for k in range(6):
            pltpu.make_async_copy(mine[k], dsts[k], li.at[k]).start()

    def ship(theirs):
        for k in range(6):
            remote(theirs[k], dsts[k], ss.at[k], sr.at[k], core=other).start()

    pl.when(c == 0)(lambda: load(gates))
    pl.when(c == 1)(lambda: load(outs))

    barrier = pltpu.get_barrier_semaphore()
    for k in (1, -1, 2, -2):
        pl.semaphore_signal(barrier, inc=1, device_id={"z": zat(k)}, device_id_type=MESH)
    for k in (1, -1):
        pl.semaphore_signal(barrier, inc=1, device_id={"x": xat(k)}, device_id_type=MESH)
        pl.semaphore_signal(barrier, inc=1, device_id={"tp": yat(k)}, device_id_type=MESH)
    pl.semaphore_signal(barrier, inc=1, device_id={"core": other}, device_id_type=MESH)

    at = lax.broadcasted_iota(jnp.int32, (low_rank, low_rank), 0)
    to = lax.broadcasted_iota(jnp.int32, (low_rank, low_rank), 1)
    source = ((to >> 3) & 3) * 128 + ((to >> 7) & 3) * 32 + ((to >> 5) & 3) * 8 + (to & 7)
    by_owner = jnp.where(at == source, 1.0, 0.0).astype(BF)

    pl.semaphore_wait(barrier, 9)

    pl.when(c == 0)(lambda: ship(outs))
    pl.when(c == 1)(lambda: ship(gates))

    def arrived(k):
        ref = dsts[k]
        pltpu.make_async_copy(gates[k], ref, li.at[k]).wait()
        remote(ref, ref, ss.at[k], sr.at[k], core=other).wait_recv()

    def gather(g, buf):
        zs, zr, xs, xr, os, orr = g_zs.at[g], g_zr.at[g], g_xs.at[g], g_xr.at[g], g_os.at[g], g_or.at[g]

        def got(ref, sem):
            remote(ref, ref, zs, sem, z=zat(1)).wait_recv()

        def zof(i):
            d = (i + 1) // 2
            return lax.rem(z + ZN + (1 - 2 * lax.rem(i, 2)) * d, ZN)

        def zsends(s):
            for sign, far in ((1, ZN // 2), (-1, ZN // 2 - 1)):
                src = buf.at[zat(-sign * 2 * s), x]
                for k in (2, 1):
                    if 2 * s + k <= far:
                        i = block_id(sign, 2 * s + k)
                        remote(src, src, zs, zr.at[(i - 1) // 2], z=zat(sign * k)).start()

        def zwait(k):
            got(buf.at[0:2, x] if k < 7 else buf.at[0, x], zr.at[k])

        def each(f, lo, hi):
            def body(i, _):
                f(i)
                return 0
            lax.fori_loop(lo, hi, body, 0)

        groups = ((0, 1), (1, 5), (5, 9), (9, 13), (13, 16))

        def forward(n):
            def one(i):
                ref = buf.at[zof(i), x]
                remote(ref, ref, xs, xr.at[n], x=xat(1)).start()
                remote(ref, ref, xs, xr.at[n], x=xat(-1)).start()
                if n == 4:
                    remote(ref, ref, os, orr, x=xat(2)).start()
            each(one, *groups[n])

        def relay(n):
            def one(i):
                zz = zof(i)
                a, b = buf.at[zz, xat(-1), pl.ds(0, 16)], buf.at[zz, xat(1), pl.ds(16, 16)]
                remote(a, a, os, orr, x=xat(1)).start()
                remote(b, b, os, orr, x=xat(-1)).start()
            lo, hi = groups[n]
            got(buf.at[0:2, 0] if n == 0 else buf.at[0:2], xr.at[n])
            each(one, lo, hi)

        def along_z(s):
            if s > 0:
                zwait(2 * s - 1)
            zsends(s)

        def along_x(n):
            if n > 0:
                zwait(2 * n - 2)
            if n == 4:
                zwait(7)
            forward(n)

        def opposite():
            got(buf.at[0:6, 0], xr.at[4])
            got(buf.at[0:4], orr)

        def finish():
            remote(buf.at[0:15, 0], buf.at[0:15, 0], zs, zr.at[0], z=zat(1)).wait_send()
            remote(buf.at[0:8], buf.at[0:8], xs, zr.at[0], z=zat(1)).wait_send()
            remote(buf.at[0:4], buf.at[0:4], os, zr.at[0], z=zat(1)).wait_send()

        return along_z, along_x, relay, opposite, finish

    Az, Ax, Ar, Ao, a_finish = gather(0, BB.at[c, 0])
    Bz, Bx, Br, Bo, b_finish = gather(1, BB.at[c, 1])
    Mz, Mx, Mr, Mo, m_finish = gather(2, MB.at[c])
    half = low_rank // 2

    arrived(0)
    ordered = jnp.dot(BS[...].reshape(32, low_rank), by_owner, preferred_element_type=F32).astype(BF)
    BB[c, 0, z, x] = ordered[:, :half]
    BB[c, 1, z, x] = ordered[:, half:]
    for s in range(4):
        Az(s)
        Ax(s)
        if s >= 2:
            Ar(s - 2)
        Bz(s)
        if s >= 1:
            Bx(s - 1)
    Ax(4)
    Ar(2)
    Ar(3)
    Bx(3)
    Br(0)
    arrived(3)
    MB[c, z, x] = MS[...].reshape(32, inner).astype(BF)
    Mz(0)
    Bx(4)
    Br(1)
    Br(2)
    Ao()
    arrived(1)

    W = low_rank // NC
    tokens = 512

    def y_copies(u):
        ref = PT.at[y, u]
        return [
            remote(ref, ref, y_s, y_r.at[0, u], tp=yat(1)),
            remote(ref, ref, y_s, y_r.at[1, u], tp=yat(-1)),
        ]

    def project(h):
        basis = BB[c, h].reshape(ZN * XN * 32, half)
        proj = jnp.dot(X[...].reshape(tokens, -1), basis, preferred_element_type=F32).T.astype(BF)
        for k in range(NC // 2):
            PT[y, h * (NC // 2) + k] = proj[k * W : (k + 1) * W]

    def send_projected(u):
        for copy in y_copies(u):
            copy.start()

    def y_relays(u):
        left, right = PT.at[yat(-1), u], PT.at[yat(1), u]
        a, b = PT.at[yat(-1), u, pl.ds(0, W // 2)], PT.at[yat(1), u, pl.ds(W // 2, W // 2)]
        return (
            remote(left, left, y_s, y_r.at[0, u], tp=yat(1)),
            remote(right, right, y_s, y_r.at[1, u], tp=yat(-1)),
            remote(a, a, yo_s, yo_r.at[u], tp=yat(1)),
            remote(b, b, yo_s, yo_r.at[u], tp=yat(-1)),
        )

    def y_stage(u):
        l, r, a, b = y_relays(u)
        l.wait_recv()
        a.start()
        r.wait_recv()
        b.start()

    def rx_copies(u):
        return [
            remote(LB.at[u, xat(d)], XR.at[u, d - 1], rx_s, rx_r.at[u], x=xat(d))
            for d in (2, 3, 1)
        ]

    def term(k, u):
        rows = pl.ds(pl.multiple_of(k * 256, 256), 256)
        return sum(
            jnp.dot(PT[k, u, :, h * 256 : (h + 1) * 256], C[h, rows], preferred_element_type=F32)
            for h in range(2)
        )

    def near_stage(u):
        LP[...] = term(y, u) + term(yat(1), u) + term(yat(-1), u)

    def low_stage(u):
        ref = PT.at[yat(2), u]
        remote(ref, ref, yo_s, yo_r.at[u], tp=yat(1)).wait_recv()
        total = LP[...] + term(yat(2), u)
        LB[u] = total.reshape(XN, ZQ, OWN, inner).astype(BF)
        for copy in rx_copies(u):
            copy.start()

    def rz_copy(u, q):
        to = q * NC + u
        return remote(ZS.at[u, q], ZR.at[z], rz_s, rz_r, z=to)

    def rx_stage(u):
        total = LB[u, x].astype(F32)
        remote(XR.at[u], XR.at[u], rx_s, rx_r.at[u], x=xat(1)).wait_recv()
        for d in range(3):
            total += XR[u, d].astype(F32)
        ZS[u] = total.astype(BF)
        for q in range(ZQ):
            pl.when(z != q * NC + u)(lambda: rz_copy(u, q).start())

    zq = z // NC

    def az_copy(u, d):
        ref = RAW.at[c, u, x, zq]
        return remote(ref, ref, az_s, az_r.at[u], z=zat(d))

    def pm_copy():
        return remote(NM.at[other], MO.at[pl.ds(2 * c, 2)], pm_s, pm_r, core=other)

    def rz_stage(u):
        @pl.when(lax.rem(z, NC) == u)
        def _():
            def add(d, total):
                return total + ZR[zat(d)].astype(F32)

            remote(ZR.at[0:15], ZR.at[0:15], rz_s, rz_r, z=zat(1)).wait_recv()
            low = lax.fori_loop(1, ZN, add, ZS[u, zq].astype(F32))
            raws = []
            for h in range(2):
                part = low[4 * h : 4 * h + 4]
                first = 0.9 * FS[0, h] + 0.1 * part
                second = 0.95 * FS[1, h] + 0.05 * part * part
                NM[h, 0] = first
                NM[h, 1] = second
                raws.append(first / jnp.sqrt(second))
            RAW[c, u, x, zq] = jnp.concatenate(raws, axis=0).astype(BF)

            def send(k, _):
                az_copy(u, ZN // 2 + (k + 1) // 2 * (1 - 2 * lax.rem(k, 2))).start()
                return 0

            lax.fori_loop(0, ZN - 1, send, 0)
            pm_copy().start()
            MO[pl.ds(2 * c, 2)] = NM[c]

    def ax_copies(u):
        ref = RAW.at[c, u, x]
        return [
            remote(ref, ref, ax_s, ax_r.at[u], x=xat(d)) for d in (2, 3, 1)
        ]

    def az_stage(u):
        def landed(n):
            ref = RAW.at[c, u, x, pl.ds(0, n)]
            remote(ref, ref, az_s, az_r.at[u], z=zat(1)).wait_recv()

        pl.when(lax.rem(z, NC) == u)(lambda: landed(ZQ - 1))
        pl.when(lax.rem(z, NC) != u)(lambda: landed(ZQ))
        for copy in ax_copies(u):
            copy.start()

    def ad_copy(u):
        ref = RAW.at[c, u]
        return remote(ref, ref, ad_s, ad_r.at[u], core=other)

    def ax_stage(u):
        ref = RAW.at[c, u, pl.ds(0, 3)]
        remote(ref, ref, ax_s, ax_r.at[u], x=xat(1)).wait_recv()
        ad_copy(u).start()

    def ad_stage(u):
        ref = RAW.at[other, u]
        remote(ref, ref, ad_s, ad_r.at[u], core=other).wait_recv()

    project(0)
    send_projected(0)
    send_projected(1)
    Br(3)
    Mz(1)
    Mx(0)
    Mx(1)
    whole = [
        remote(BB.at[c], BB.at[c], d_s.at[0], d_r.at[0], core=other),
        remote(MB.at[c], MB.at[c], d_s.at[1], d_r.at[1], core=other),
    ]
    Bo()
    project(1)
    Mz(2)
    Mx(2)
    y_stage(0)
    send_projected(2)
    whole[0].start()
    send_projected(3)
    Mr(0)
    y_stage(1)
    Mr(1)
    Mz(3)
    Mx(3)
    for k in (2, 4, 5):
        arrived(k)
    near_stage(0)
    low_stage(0)
    near_stage(1)
    y_stage(2)
    Mr(2)
    low_stage(1)
    near_stage(2)
    y_stage(3)
    rx_stage(0)
    low_stage(2)
    near_stage(3)
    low_stage(3)
    Mx(4)
    rx_stage(1)
    Mr(3)
    rx_stage(2)
    rx_stage(3)
    for u in range(NC):
        rz_stage(u)
    Mo()
    whole[1].start()
    remote(BB.at[other], BB.at[other], d_s.at[0], d_r.at[0], core=other).wait_recv()

    def turn_basis(t, _):
        rows = pl.ds(pl.multiple_of(t * 256, 256), 256)
        for h in range(2):
            BT[h, :, rows] = BB[1, h, pl.ds(t * 2, 2)].reshape(256, half).T
        return 0

    lax.fori_loop(0, 8, turn_basis, 0)
    az_stage(0)
    az_stage(1)
    landed = remote(MB.at[other], MB.at[other], d_s.at[1], d_r.at[1], core=other)
    pl.when(c == 0)(landed.wait_recv)

    def turn(t, _):
        rows = pl.ds(pl.multiple_of(t * 256, 256), 256)
        N[:, rows] = MB[1, pl.ds(t * 2, 2)].reshape(256, inner).T
        return 0

    lax.fori_loop(0, 8, turn, 0)
    az_stage(2)
    ax_stage(0)
    az_stage(3)
    ax_stage(1)

    def raw_half(m, h):
        return RAW[m, h * (NC // 2) : (h + 1) * (NC // 2)].reshape(half, inner)

    def gate_half(h):
        def some(t, _):
            zz, rows = pl.ds(t * 8, 8), pl.ds(pl.multiple_of(t * 1024, 1024), 1024)
            part = jnp.dot(
                BB[0, h, zz].reshape(1024, half), raw_half(0, h), preferred_element_type=F32
            )
            U[rows] = part if h == 0 else U[rows] + part
            return 0

        lax.fori_loop(0, 2, some, 0)

    def out_half(h):
        RT[...] = raw_half(1, h).T

        def some(t, _):
            rows = pl.ds(pl.multiple_of(t * 1024, 1024), 1024)
            part = jnp.dot(RT[...], BT[h, :, rows], preferred_element_type=F32)
            V[:, rows] = part if h == 0 else V[:, rows] + part
            return 0

        lax.fori_loop(0, 2, some, 0)

    pl.when(c == 0)(lambda: gate_half(0))
    pl.when(c == 1)(lambda: out_half(0))
    ax_stage(2)
    ad_stage(0)
    ad_stage(1)
    pl.when(c == 0)(lambda: out_half(0))
    pl.when(c == 1)(lambda: gate_half(0))

    def squares(m, u):
        r = RAW[m, u].reshape(W, inner).astype(F32)
        r = (r * r).reshape(W // 8, 8, inner).sum(axis=0)
        return sum(r[:, k * 128 : (k + 1) * 128] for k in range(inner // 128))

    total = jnp.zeros((8, 128), F32)
    for u in range(NC // 2):
        total += squares(0, u) + squares(1, u)
    ad_stage(2)
    total += squares(0, 2) + squares(1, 2)
    ax_stage(3)
    total += squares(c, 3)
    ad_stage(3)
    SQ[y] = total + squares(other, 3)

    def sq_copy(d):
        return remote(SQ.at[y], SQ.at[y], sq_s, sq_r, tp=yat(d))

    for d in (1, 2, 3):
        sq_copy(d).start()

    gate_half(1)
    out_half(1)
    own_rows = pl.ds(pl.multiple_of(c * 16, 16), 16)
    OR[...] = sum(
        jnp.dot(BB[1, h, z, x, own_rows], raw_half(1, h), preferred_element_type=F32)
        for h in range(2)
    )
    remote(SQ.at[0:3], SQ.at[0:3], sq_s, sq_r, tp=yat(1)).wait_recv()

    pl.when(c == 1)(landed.wait_recv)
    remote(NM.at[c], NM.at[c], pm_s, pm_r, core=other).wait_recv()

    for k in range(6):
        remote(dsts[k], dsts[k], ss.at[k], sr.at[k], core=other).wait_send()
    a_finish()
    b_finish()
    m_finish()
    for copy in whole:
        copy.wait_send()
    for ref, sem in ((PT.at[0:2], y_s), (PT.at[0], yo_s), (XR, rx_s), (XR, ax_s), (LB, ad_s)):
        remote(ref, ref, sem, y_r.at[0, 0], tp=yat(1)).wait_send()
    fifteen = ZR.at[0:15]
    remote(fifteen, fifteen, rz_s, rz_r, z=zat(1)).wait_send()
    remote(fifteen, fifteen, az_s, rz_r, z=zat(1)).wait_send()
    pm_copy().wait_send()
    remote(SQ.at[0:3], SQ.at[0:3], sq_s, sq_r, tp=yat(1)).wait_send()


def finish(
    low_rank, inner,
    MB, U, V, N, OR, SQ, MO, gm, om,
    gm_out, om_out, gcopy, ocopy, gf_out, gs_out, of_out, os_out,
    GO, OO, GMO, OMO, out_s, few_s,
):
    z, x, c = (lax.axis_index(a) for a in ("z", "x", "core"))
    total = jnp.sum(SQ[0] + SQ[1] + SQ[2] + SQ[3])
    full = GO.shape[0]
    few = [
        pltpu.make_async_copy(MO.at[k], ref, few_s.at[k])
        for k, ref in enumerate((gf_out, gs_out, of_out, os_out))
    ]
    for copy in few:
        copy.start()
    scale_t = 0.25 * lax.rsqrt(
        jnp.full((1, full), total, F32) / (2.0 * low_rank * inner * YN) + 1e-06
    )
    scale = scale_t[:, :inner]
    TILE = 256

    def gate_out(t):
        rows = pl.ds(pl.multiple_of(t * TILE, TILE), TILE)
        return pltpu.make_async_copy(GO.at[rows], gcopy.at[rows], out_s.at[0, t])

    def out_out(t):
        rows = pl.ds(pl.multiple_of(t * 64, 64), 64)
        return pltpu.make_async_copy(OO.at[rows], ocopy.at[rows], out_s.at[1, t])

    def tile(t, _):
        zz = pl.ds(t * 2, 2)
        rows = pl.ds(pl.multiple_of(t * TILE, TILE), TILE)
        GO[rows] = (MB[0, zz].reshape(TILE, inner).astype(F32) - scale * U[rows]).astype(BF)
        gate_out(t).start()
        rows = pl.ds(pl.multiple_of(t * 64, 64), 64)
        OO[rows] = (N[rows].astype(F32) - scale_t * V[rows]).astype(BF)
        out_out(t).start()
        return 0

    mine = pl.ds(pl.multiple_of((z * XN + x) * 32 + c * 16, 16), 16)
    GMO[...] = gm[...] - scale * U[mine]
    OMO[...] = om[...] - scale * OR[...]
    few += [
        pltpu.make_async_copy(GMO, gm_out, few_s.at[4]),
        pltpu.make_async_copy(OMO, om_out, few_s.at[5]),
    ]
    for copy in few[4:]:
        copy.start()
    lax.fori_loop(0, 8, tile, 0)
    mine = pl.ds(pl.multiple_of((z * XN + x) * 32 + c * 16, 16), 16)
    def done(t, _):
        gate_out(t).wait()
        out_out(t).wait()
        return 0

    lax.fori_loop(0, 8, done, 0)
    for copy in few:
        copy.wait()


def on_device(
    block_input, gate_cotangent, gated_state, mixer_cotangent, gate_basis, out_basis,
    gate_master, out_master, gate_first, gate_second, out_first, out_second,
):
    low_rank = gate_basis.shape[1]
    inner = gate_first.shape[1]
    rows = gate_basis.shape[0]

    out_t = out_master.T
    D = pltpu.SemaphoreType.DMA
    vm = pltpu.VMEM
    full = rows * ZN * XN * 2
    W = low_rank // NC
    held = (
        jax.ShapeDtypeStruct((2, ZN, XN, 32, inner), BF),
        jax.ShapeDtypeStruct((full, inner), F32),
        jax.ShapeDtypeStruct((inner, full), F32),
        jax.ShapeDtypeStruct((inner, full), BF),
        jax.ShapeDtypeStruct((rows, inner), F32),
        jax.ShapeDtypeStruct((YN, 8, 128), F32),
        jax.ShapeDtypeStruct((4, *gate_first.shape), F32),
    )
    vmem = pl.BlockSpec(memory_space=pltpu.VMEM)
    hbm = pl.BlockSpec(memory_space=pltpu.HBM)
    held = pl.pallas_call(
        functools.partial(kernel, low_rank, inner),
        out_shape=held,
        in_specs=[hbm] * 12,
        out_specs=[vmem] * 7,
        scratch_shapes=[
            vm((2, 2, ZN, XN, 32, low_rank // 2), BF),
            vm((2, NC, XN, ZQ, OWN, inner), BF),
            vm((2, low_rank // 2, full), BF),
            vm((inner, low_rank // 2), BF),
            vm((W, inner), F32),
            vm((2, 256, full), BF),
            vm((2, 1024, inner), BF),
            vm((2, rows, low_rank), BF),
            vm((2, rows, inner), F32),
            vm((YN, NC, W, 512), BF),
            vm((NC, XN, ZQ, OWN, inner), BF),
            vm((NC, 3, ZQ, OWN, inner), BF),
            vm((NC, ZQ, OWN, inner), BF),
            vm((ZN, OWN, inner), BF),
            vm((2, 2, 4, inner), F32),
            vm((2, 2, 4, inner), F32),
            D((6,)), D((6,)), D((6,)),
            D((3,)), D((3, NID // 2)), D((3,)), D((3, 5)), D((3,)), D((3,)),
            D((2,)), D((2,)),
            D, D((2, NC)), D, D((NC,)),
            D, D((NC,)), D, D,
            D, D((NC,)), D, D((NC,)), D, D((NC,)),
            D, D, D, D,
        ],
        compiler_params=pltpu.CompilerParams(
            collective_id=0, has_side_effects=True, vmem_limit_bytes=LIMIT1
        ),
        name="moment_update",
    )(
        *(pltpu.with_memory_space_constraint(a, pltpu.HBM) for a in (
            block_input, gate_cotangent, gated_state, mixer_cotangent, gate_basis, out_basis,
            gate_master, out_t, gate_first, gate_second, out_first, out_second,
        ))
    )
    outs = (
        jax.ShapeDtypeStruct((rows, inner), F32),
        jax.ShapeDtypeStruct((rows, inner), F32),
        jax.ShapeDtypeStruct((full, inner), BF),
        jax.ShapeDtypeStruct((inner, full), BF),
    ) + (jax.ShapeDtypeStruct(gate_first.shape, F32),) * 4
    res = pl.pallas_call(
        functools.partial(finish, low_rank, inner),
        out_shape=outs,
        in_specs=[vmem] * 9,
        out_specs=[hbm] * 8,
        scratch_shapes=[
            vm((full, inner), BF), vm((inner, full), BF), vm((rows, inner), F32), vm((rows, inner), F32),
            D((2, 8)), D((6,)),
        ],
        compiler_params=pltpu.CompilerParams(vmem_limit_bytes=LIMIT2),
        name="apply_step",
    )(*held, gate_master, out_t)
    return (res[0], res[1].T, *res[2:])


def solution(mesh):
    finer = Mesh(mesh.devices.reshape(ZN, XN, 2, mesh.shape["tp"]), FS_TP)
    in_specs = (
        P(FS_TP, None), P(FSN, "tp"), P(FSN, "tp"), P(FS_TP, None), P(FSN, None), P(FSN, None),
        P(FSN, "tp"), P("tp", FSN), P(FSN, "tp"), P(FSN, "tp"), P(FSN, "tp"), P(FSN, "tp"),
    )
    out_specs = (
        P(FSN, "tp"), P("tp", FSN), P(None, "tp"), P("tp", None),
        P(FSN, "tp"), P(FSN, "tp"), P(FSN, "tp"), P(FSN, "tp"),
    )
    return jax.shard_map(
        on_device, mesh=finer, in_specs=in_specs, out_specs=out_specs, check_vma=False
    )
```
